32 devices in a mesh: sp: 8 (over z, y), tp: 4 (over x, core).
Axes of the slice: x: 2, y: 2, z: 4, core: 2. Of those that a mesh axis runs over, the one named last changes fastest.
Arguments:
- hidden: bfloat16 [3072, 4096], P('sp', 'tp'), may hold values from -6 to 6
- doc_ids: int32 [3072], P('sp'), may hold values from 0 to 3, never falling along the last dimension, each value on 1 to 1536 neighbouring positions
- norm_gain: float32 [3, 4096], replicated, may hold values from 0.1 to 1.9
- w_value: bfloat16 [3, 4096, 2048], P(None, 'sp', 'tp'), may hold values from -0.09375 to 0.09375
- w_gate: bfloat16 [3, 4096, 2048], P(None, 'sp', 'tp'), may hold values from -0.09375 to 0.09375
- conv_taps: float32 [3, 31, 2048], P(None, None, 'tp'), may hold values from -1 to 1
- conv_bias: float32 [3, 2048], P(None, 'tp'), may hold values from -3 to 3
- chan_gain: float32 [3, 2048], P(None, 'tp'), may hold values from 0.1 to 1.9
- chan_bias: float32 [3, 2048], P(None, 'tp'), may hold values from -3 to 3
- w_out: bfloat16 [3, 2048, 4096], P(None, 'sp', 'tp'), may hold values from -0.125 to 0.125
Outputs:
- result: bfloat16 [3072, 4096], P('sp', 'tp')
The draws below stay inside these ranges and needn't reach their ends.
Inputs may be any that keep to these rules, and one draw needn't show every extreme that they name: `doc_ids`: document numbers never fall along the sequence; each document has 1 to 1536 positions and one has exactly that many.
All inputs are finite; a program needn't handle non-finite values.
Results may differ from the reference program's by a relative error of at most 0.013.
Values may be sent and summed in bfloat16 or wider, within the bound.
A program may use at most 128 MiB of HBM per device.

```python
import math
import jax
import jax.numpy as jnp
import numpy as np
from jax import lax

D = 4096
C = 2048
CONV_WIDTH = 31
LAYERS = 3
TOK_DEV = 384
TOKENS = 3072
DOCS = 4


def levels(own_key, extent, shards, low, largest):
    level = 1.0
    for position, shards_of in shards:
        steps = jax.random.uniform(jax.random.fold_in(jax.random.fold_in(own_key, 6), position), (shards_of,), jnp.float32, low / len(shards), largest / len(shards))
        level = level * jnp.repeat(jnp.exp(steps), extent[position] // shards_of).reshape((-1,) + (1,) * (len(extent) - 1 - position))
    return level


def profile(count, total, most, lean):
    loads = [(1 << 20) // math.isqrt(grade ** lean) + 1 for grade in range(2, count + 1)]
    rest, counts = total - most - (count - 1), [1] * (count - 1)
    while rest > 0:
        free = [i for i in range(count - 1) if counts[i] < most]
        mass, left = sum([loads[i] for i in free]), rest
        for i in free:
            more = min(most - counts[i], max(1, left * loads[i] // mass), rest)
            counts[i] = counts[i] + more
            rest = rest - more
    return np.array([most] + counts)


def uneven_parts(stream_key, amount, total, limit, lean):
    if amount == 2:
        one = jax.random.randint(stream_key, (), max(1, total - limit), min(limit, total - 1) + 1)
        return jnp.stack([one, total - one])
    lengths = jnp.asarray(profile(amount, total, limit, lean), jnp.int32)
    twos = (amount - 1) // 2
    donor, taker = lengths[1:1 + 2 * twos:2], lengths[2:2 + 2 * twos:2]
    margin = jnp.minimum(donor - 1, limit - taker)
    passed = jax.random.randint(jax.random.fold_in(stream_key, 1), (twos,), 0, 1 << 20) % (margin + 1)
    lengths = lengths.at[1:1 + 2 * twos:2].set(donor - passed).at[2:2 + 2 * twos:2].set(taker + passed)
    return lengths[jax.random.permutation(jax.random.fold_in(stream_key, 2), amount)]


def scatter_about(own_key, shape, scale, reach, pieces=(), dtype=jnp.bfloat16):
    loudness = levels(own_key, shape, pieces, -0.22, 0.18) if pieces else 1.0
    drawn = jax.random.normal(own_key, shape, jnp.float32) * scale * loudness
    return jnp.minimum(jnp.maximum(drawn, -reach), reach).astype(dtype)


def setup_inputs(seed: int = 0) -> dict:
    arg_keys = jax.random.split(jax.random.key(seed), 11)
    hidden = scatter_about(arg_keys[0], (TOKENS, D), 1.0, 6.0, ((0, 8), (1, 4)))
    doc_ids = jnp.searchsorted(jnp.cumsum(uneven_parts(arg_keys[1], DOCS, TOKENS, 4 * TOK_DEV, 0)), jnp.arange(TOKENS), side="right").astype(jnp.int32)
    norm_gain = jnp.clip(1.0 + 0.18 * jax.random.normal(arg_keys[2], (LAYERS, D), jnp.float32), 0.1, 1.9)
    w_value = scatter_about(arg_keys[3], (LAYERS, D, C), D ** -0.5, 0.09375, ((1, 8), (2, 4)))
    w_gate = scatter_about(arg_keys[4], (LAYERS, D, C), D ** -0.5, 0.09375, ((1, 8), (2, 4)))
    conv_taps = scatter_about(arg_keys[5], (LAYERS, CONV_WIDTH, C), CONV_WIDTH ** -0.5, 1.0, ((2, 4),), jnp.float32)
    conv_bias = scatter_about(arg_keys[6], (LAYERS, C), 0.5, 3.0, ((1, 4),), jnp.float32)
    chan_gain = jnp.clip(1.0 + 0.18 * jax.random.normal(arg_keys[7], (LAYERS, C), jnp.float32), 0.1, 1.9)
    chan_bias = scatter_about(arg_keys[8], (LAYERS, C), 0.5, 3.0, ((1, 4),), jnp.float32)
    w_out = scatter_about(arg_keys[9], (LAYERS, C, D), C ** -0.5, 0.125, ((1, 8), (2, 4)))
    return {"hidden": hidden, "doc_ids": doc_ids, "norm_gain": norm_gain, "w_value": w_value, "w_gate": w_gate, "conv_taps": conv_taps, "conv_bias": conv_bias, "chan_gain": chan_gain, "chan_bias": chan_bias, "w_out": w_out}


def one_layer(hidden, doc_ids, norm_gain, w_value, w_gate, conv_taps, conv_bias, chan_gain, chan_bias, w_out):
    width = conv_taps.shape[0]
    length = hidden.shape[0]
    xfloat = hidden.astype(jnp.float32)
    scale = lax.rsqrt(lax.optimization_barrier(jnp.mean(xfloat * xfloat, axis=-1, keepdims=True)) + 1e-06)
    normed = (xfloat * scale * norm_gain).astype(jnp.bfloat16)
    value = jnp.dot(normed, w_value, preferred_element_type=jnp.float32)
    gate = jnp.dot(normed, w_gate, preferred_element_type=jnp.float32)
    glu = (value * jax.nn.sigmoid(gate)).astype(jnp.bfloat16)
    padded = jnp.concatenate([jnp.zeros((width - 1, glu.shape[1]), jnp.float32), glu.astype(jnp.float32)], axis=0)
    seg_pad = jnp.concatenate([jnp.full((width - 1,), -1, jnp.int32), doc_ids.astype(jnp.int32)], axis=0)
    conv = jnp.zeros(glu.shape, jnp.float32) + conv_bias
    for index in range(width):
        source = padded[index:index + length]
        keep = (seg_pad[index:index + length] == doc_ids)[:, None]
        conv = conv + jnp.where(keep, source * conv_taps[index], 0.0)
    mean_val = lax.optimization_barrier(jnp.mean(conv, axis=-1, keepdims=True))
    var_val = lax.optimization_barrier(jnp.mean(conv * conv, axis=-1, keepdims=True)) - mean_val * mean_val
    mixed = jax.nn.silu((conv - mean_val) * lax.rsqrt(var_val + 1e-05) * chan_gain + chan_bias).astype(jnp.bfloat16)
    return (xfloat + jnp.dot(mixed, w_out, preferred_element_type=jnp.float32)).astype(jnp.bfloat16)

def reference(hidden, doc_ids, norm_gain, w_value, w_gate, conv_taps, conv_bias, chan_gain, chan_bias, w_out):
    state = hidden
    for layer in range(LAYERS):
        state = one_layer(state, doc_ids, norm_gain[layer], w_value[layer], w_gate[layer], conv_taps[layer], conv_bias[layer], chan_gain[layer], chan_bias[layer], w_out[layer])
    return state
```

```python
import functools
import math

import jax
import jax.numpy as jnp
from jax import lax
from jax.experimental import pallas as pl
from jax.experimental.pallas import tpu as pltpu
from jax.sharding import PartitionSpec as P

MESH = pl.DeviceIdType.MESH
HALO = 32
ROWS = 64


def grid_of(size):
    inner = max(d for d in range(1, math.isqrt(size) + 1) if size % d == 0)
    return size // inner, inner


def kernel(
    dims,
    hid,
    pos,
    ngain,
    wv,
    wg,
    taps,
    cbias,
    cgain,
    chbias,
    wo,
    out,
    wp_buf,
    wo_buf,
    rp_buf,
    ro_buf,
    xg,
    xn,
    mg,
    prod,
    branch,
    glu,
    conv,
    state,
    final,
    tail,
    halo,
    stat,
    stat_out,
    stat_in,
    cols,
    loc_sem,
    z_recv,
    r_recv,
    y_recv,
    z_send,
    y_send,
    h_recv,
    h_send,
    m_recv,
    m_send,
    s_recv,
    s_send,
    t_recv,
    t_send,
    f_sem,
):
    Z, Y, X, T, D, C, LAYERS, WIDTH = dims
    S = 4 * X
    cs, ds_ = C // S, D // S
    parts = 2 * LAYERS
    nx, ny = X - 1, Y - 1

    spi, tpi = lax.axis_index("sp"), lax.axis_index("tp")
    z, y, x, c = spi // Y, spi % Y, tpi // 2, tpi % 2
    zn = z + 1 - 2 * (z % 2)
    zh, ko = z // 2, z % 2
    inner = ((z + 1) // 2) % 2
    h = 1 - inner
    zin = inner * z + h * zn
    zout = h * z + inner * zn
    me = (x * 2 + c) * 2 + h

    def dev(zz, yy, xx, cc):
        return (zz * Y + yy, xx * 2 + cc)

    partner = dev(z, y, x, 1 - c)
    zpeer = dev(zn, y, x, c)
    mid = dev(Z - 1 - z, y, x, c)

    def send(src, dst, ssem, rsem, device):
        pltpu.make_async_remote_copy(
            src_ref=src, dst_ref=dst, send_sem=ssem, recv_sem=rsem,
            device_id=device, device_id_type=MESH,
        ).start()

    def recv_wait(ref, sem):
        pltpu.make_async_remote_copy(
            src_ref=ref, dst_ref=ref, send_sem=sem, recv_sem=sem,
            device_id=partner, device_id_type=MESH,
        ).wait_recv()

    def send_wait(ref, sem):
        pltpu.make_async_remote_copy(
            src_ref=ref, dst_ref=ref, send_sem=sem, recv_sem=sem,
            device_id=partner, device_id_type=MESH,
        ).wait_send()

    def lanes(start, size):
        return pl.ds(pl.multiple_of(start, 128), size)

    def block(q, b):
        return (wo_buf if q % 2 else wp_buf).at[q // 2, b]

    def relay(q, i):
        return (ro_buf if q % 2 else rp_buf).at[q // 2, i]

    def own_pieces(q, half, dst):
        l = q // 2
        if q % 2:
            return [(wo.at[l, :, lanes(half * ds_, ds_)], dst)]
        return [
            (wv.at[l, :, lanes(half * cs, cs)], dst.at[:, pl.ds(0, cs)]),
            (wg.at[l, :, lanes(half * cs, cs)], dst.at[:, pl.ds(cs, cs)]),
        ]

    def own_send(q, half, dst, ssem, rsem, device):
        for src, part in own_pieces(q, half, dst):
            send(src, part, ssem, rsem, device)

    def y_spread(q, zb):
        b = zb * Y + y
        for j in range(1, Y):
            send(block(q, b), block(q, b), y_send.at[q, zb, j - 1], y_recv.at[q, zb, j - 1],
                 dev(z, (y + j) % Y, x, c))

    def start_part(q):
        mine = block(q, z * Y + y)
        own_send(q, 1 - h, mine, z_send.at[q, 0], z_recv.at[q, 0], zpeer)

        @pl.when(inner == 0)
        def _():
            own_send(q, h, relay(q, 1), z_send.at[q, 1], r_recv.at[q, 1], zpeer)

        @pl.when(inner == 1)
        def _():
            own_send(q, 1 - h, relay(q, 0), z_send.at[q, 1], r_recv.at[q, 0], mid)
            own_send(q, h, mine, z_send.at[q, 2], z_recv.at[q, 1], mid)

        for j in range(1, Y):
            own_send(q, h, mine, y_send.at[q, z, j - 1], y_recv.at[q, z, j - 1],
                     dev(z, (y + j) % Y, x, c))
        for src, part in own_pieces(q, h, mine):
            pltpu.make_async_copy(src, part, loc_sem.at[q]).start()

    def event1(q):
        recv_wait(block(q, zn * Y + y), z_recv.at[q, 0])
        y_spread(q, zn)

        @pl.when(inner == 1)
        def _():
            recv_wait(relay(q, 0), r_recv.at[q, 0])
            send(relay(q, 0), block(q, (Z - 1 - z) * Y + y), z_send.at[q, 3], z_recv.at[q, 1], zpeer)

    def event2(q):
        @pl.when(inner == 1)
        def _():
            recv_wait(relay(q, 1), r_recv.at[q, 1])
            send(relay(q, 1), relay(q, 2), z_send.at[q, 4], r_recv.at[q, 2], mid)
            near = block(q, zn * Y + y)
            send(near, near, z_send.at[q, 5], z_recv.at[q, 2], mid)

        zb = Z - 1 - zin
        recv_wait(block(q, zb * Y + y), z_recv.at[q, 1])
        y_spread(q, zb)

    def event3(q):
        @pl.when(inner == 1)
        def _():
            recv_wait(relay(q, 2), r_recv.at[q, 2])
            send(relay(q, 2), block(q, (Z - 1 - zn) * Y + y), z_send.at[q, 6], z_recv.at[q, 2], zpeer)

    def event4(q):
        zb = Z - 1 - zout
        recv_wait(block(q, zb * Y + y), z_recv.at[q, 2])
        y_spread(q, zb)

    def part_ready(q):
        mine = block(q, z * Y + y)
        pltpu.make_async_copy(mine, mine, loc_sem.at[q]).wait()
        for zb in range(Z):
            for j in range(1, Y):
                recv_wait(block(q, zb * Y + (y - j + Y) % Y), y_recv.at[q, zb, j - 1])

    def part_sent(q):
        ref = block(q, 0)
        for zb in range(Z):
            for j in range(1, Y):
                send_wait(ref, y_send.at[q, zb, j - 1])
        send_wait(ref, z_send.at[q, 0])
        send_wait(ref, z_send.at[q, 1])

        @pl.when(inner == 1)
        def _():
            for i in range(2, 7):
                send_wait(ref, z_send.at[q, i])

    class Gather:
        def __init__(self, region, recv, sent, source=None):
            self.region, self.recv, self.sent = region, recv, sent
            self.own = region(x, c, z)
            self.source = self.own if source is None else source

        def xs(self, j):
            return (x - j + X) % X

        def forward(self, ref, i, device):
            send(ref, ref, self.sent.at[i], self.recv.at[i], device)

        def first(self):
            def go(i, device):
                send(self.source, self.own, self.sent.at[i], self.recv.at[i], device)

            go(1, zpeer)
            for j in range(1, X):
                go(2 + j, dev(z, y, (x + j) % X, c))
            go(0, partner)

        def second(self):
            ref = self.region(x, c, zn)
            recv_wait(ref, self.recv.at[1])
            for j in range(1, X):
                self.forward(ref, 2 + nx + j, dev(z, y, (x + j) % X, c))
            self.forward(ref, 2, partner)

        def third(self):
            for j in range(1, X):
                ref = self.region(self.xs(j), c, z)
                recv_wait(ref, self.recv.at[2 + j])
                self.forward(ref, 2 + 2 * nx + j, partner)
            for j in range(1, X):
                ref = self.region(self.xs(j), c, zn)
                recv_wait(ref, self.recv.at[2 + nx + j])
                self.forward(ref, 2 + 3 * nx + j, partner)

        def last(self):
            recv_wait(self.region(x, 1 - c, z), self.recv.at[0])
            recv_wait(self.region(x, 1 - c, zn), self.recv.at[2])
            for j in range(1, X):
                recv_wait(self.region(self.xs(j), 1 - c, z), self.recv.at[2 + 2 * nx + j])
                recv_wait(self.region(self.xs(j), 1 - c, zn), self.recv.at[2 + 3 * nx + j])

        def drained(self):
            for i in range(3 + 4 * nx):
                send_wait(self.own, self.sent.at[i])

    def slot(xx, cc, zz):
        return (xx * 2 + cc) * 2 + 1 - ((zz + 1) // 2) % 2

    def hidden_gather(layer, k):
        if layer == 0:
            return Gather(
                lambda xx, cc, zz: xg.at[zz % 2, :, lanes((xx * 2 + cc) * 2 * ds_, 2 * ds_)],
                h_recv.at[0], h_send.at[0], hid,
            )
        return Gather(
            lambda xx, cc, zz: xg.at[k, :, lanes(slot(xx, cc, zz) * ds_, ds_)],
            h_recv.at[k], h_send.at[k], state.at[k],
        )

    def mixed_gather(k):
        return Gather(
            lambda xx, cc, zz: mg.at[k, :, lanes(slot(xx, cc, zz) * cs, cs)],
            m_recv.at[k], m_send.at[k],
        )

    def normalise(layer, k):
        gain = ngain.at[layer]

        @pl.loop(0, T // 16)
        def _(i):
            rows = pl.ds(pl.multiple_of(i * 16, 16), 16)
            v = xg[k, rows, :].astype(jnp.float32)
            scale = lax.rsqrt(jnp.mean(v * v, axis=-1, keepdims=True) + 1e-6)
            xn[rows, :] = (v * scale * gain[...][None, :]).astype(jnp.bfloat16)

    def matmul(acc, lhs, rhs, depth, count):
        acc[...] = jnp.zeros_like(acc)

        @pl.loop(0, count)
        def _(b):
            acc[...] += jnp.dot(
                lhs[:, lanes(b * depth, depth)], rhs[b], preferred_element_type=jnp.float32
            )

    def project(layer, k):
        matmul(prod, xn, wp_buf.at[layer], D // (Z * Y), Z * Y)

        @pl.loop(0, T // HALO)
        def _(i):
            rows = pl.ds(pl.multiple_of(i * HALO, HALO), HALO)
            v, g = prod[rows, 0:cs], prod[rows, cs : 2 * cs]
            r = (v * jax.nn.sigmoid(g)).astype(jnp.bfloat16)
            glu[k, pl.ds(pl.multiple_of(i * HALO + HALO, HALO), HALO), :] = r.astype(jnp.float32)

        tail[layer, k] = glu[k, T : T + HALO, :].astype(jnp.bfloat16)

    def tail_send(layer, k):
        def go(kk, device):
            send(tail.at[layer, k], halo.at[layer, kk], t_send.at[layer, k], t_recv.at[layer, kk], device)

        @pl.when(y < Y - 1)
        def _():
            go(k, dev(z, y + 1, x, c))

        if k == 0:
            @pl.when(y == Y - 1)
            def _():
                go(1, dev(z, 0, x, c))
        else:
            @pl.when((y == Y - 1) & (zh == 0))
            def _():
                go(0, dev(Z - 1 - z, 0, x, c))

    def tail_sent(layer, k):
        if k == 0:
            send_wait(tail.at[layer, k], t_send.at[layer, k])
        else:
            @pl.when((y < Y - 1) | (zh == 0))
            def _():
                send_wait(tail.at[layer, k], t_send.at[layer, k])

    def tail_recv(layer, k):
        def arrive():
            recv_wait(halo.at[layer, k], t_recv.at[layer, k])
            glu[k, 0:HALO, :] = halo[layer, k].astype(jnp.float32)

        if k == 1:
            arrive()
        else:
            @pl.when((y > 0) | (zh > 0))
            def _():
                arrive()

            @pl.when((y == 0) & (zh == 0))
            def _():
                glu[k, 0:HALO, :] = jnp.zeros((HALO, cs), jnp.float32)

    def convolve(layer, k):
        first_lane = lax.broadcasted_iota(jnp.int32, (ROWS, 128), 1) == 0

        @pl.loop(0, T // ROWS)
        def _(i):
            base = pl.multiple_of(i * ROWS, ROWS)
            near = pos[k, pl.ds(base, ROWS), :]
            total = jnp.zeros((ROWS, 128), jnp.float32)
            square = jnp.zeros((ROWS, 128), jnp.float32)
            for t in range(cs // 128):
                at = lanes(h * cs + t * 128, 128)
                span = glu[k, pl.ds(base, ROWS + HALO), t * 128 : (t + 1) * 128]
                acc = jnp.broadcast_to(cbias[layer : layer + 1, at], (ROWS, 128))
                for phase in range(8):
                    moved = span if phase == 0 else pltpu.roll(span, ROWS + HALO - phase, 0)
                    for off in range(phase, HALO + 1, 8):
                        index = off - (HALO - (WIDTH - 1))
                        if 0 <= index < WIDTH:
                            start = off - phase
                            term = moved[start : start + ROWS] * taps[layer, index : index + 1, at]
                            back = WIDTH - 1 - index
                            acc = acc + (jnp.where(near >= back, term, 0.0) if back else term)
                conv[k, pl.ds(base, ROWS), t * 128 : (t + 1) * 128] = acc
                total = total + acc
                square = square + acc * acc
            s1 = jnp.sum(total, axis=1, keepdims=True)
            s2 = jnp.sum(square, axis=1, keepdims=True)
            stat[pl.ds(base, ROWS), :] = jnp.where(first_lane, s1, s2)

        for t in range(T // 128):
            stat_out[k, :, t * 128 : (t + 1) * 128] = stat[t * 128 : (t + 1) * 128, :].T[0:8, :]

    def others():
        for xj in range(X):
            for cj in range(2):
                for zj in range(2):
                    if xj or cj or zj:
                        xx, cc = (x + xj) % X, (c + cj) % 2
                        zz, zb = (zn, zn) if zj else (z, z)
                        back = ((x - xj + X) % X, (c + cj) % 2, zz)
                        yield (xj * 2 + cj) * 2 + zj, dev(zz, y, xx, cc), slot(*back)

    def stats_send(k):
        for i, device, _ in others():
            send(stat_out.at[k], stat_in.at[k, me], s_send.at[k, i], s_recv.at[k, i], device)

    def mix(layer, k):
        for i, _, theirs in others():
            recv_wait(stat_in.at[k, theirs], s_recv.at[k, i])
        stat_in[k, me] = stat_out[k]
        total = stat_in[k, 0]
        for i in range(1, S):
            total = total + stat_in[k, i]
        for t in range(T // 128):
            tile = total[:, t * 128 : (t + 1) * 128]
            turned = jnp.concatenate([tile] * 16, axis=0).T
            mu = turned[:, 0:1] * (1.0 / C)
            var = turned[:, 1:2] * (1.0 / C) - mu * mu
            rows = slice(t * 128, (t + 1) * 128)
            cols[0, rows, :] = jnp.broadcast_to(mu, (128, 128))
            cols[1, rows, :] = jnp.broadcast_to(lax.rsqrt(var + 1e-5), (128, 128))

        @pl.loop(0, T // ROWS)
        def _(i):
            rows = pl.ds(pl.multiple_of(i * ROWS, ROWS), ROWS)
            mu, scale = cols[0, rows, :], cols[1, rows, :]
            for t in range(cs // 128):
                at = lanes(h * cs + t * 128, 128)
                v = (conv[k, rows, t * 128 : (t + 1) * 128] - mu) * scale
                v = v * cgain[layer : layer + 1, at] + chbias[layer : layer + 1, at]
                mg[k, rows, lanes(me * cs + t * 128, 128)] = jax.nn.silu(v).astype(jnp.bfloat16)

    def stats_sent(k):
        for i, _, _ in others():
            send_wait(stat_out.at[k], s_send.at[k, i])

    def contract(layer, k):
        matmul(branch, mg.at[k], wo_buf.at[layer], C // (Z * Y), Z * Y)
        state[k] = (state[k].astype(jnp.float32) + branch[...]).astype(jnp.bfloat16)

    own0 = xg.at[ko, :, lanes((x * 2 + c) * 2 * ds_, 2 * ds_)]
    local = pltpu.make_async_copy(hid, own0, f_sem.at[0])
    local.start()
    start_part(0)
    gather0 = hidden_gather(0, 0)
    gather0.first()
    event1(0)
    event2(0)
    gather0.second()
    event3(0)
    start_part(1)
    event4(0)
    gather0.third()
    local.wait()

    for layer in range(LAYERS):
        p_next, o_now, o_next = 2 * layer + 2, 2 * layer + 1, 2 * layer + 3
        more = layer + 1 < LAYERS
        event1(o_now)
        event2(o_now)
        for k in range(2):
            gh = gather0 if layer == 0 else hidden_gather(layer, k)
            if layer or k == 0:
                gh.last()
            if layer == 0:
                if k == 0:
                    for kk in range(2):
                        state[kk] = xg[kk, :, lanes(me * ds_, ds_)]
            normalise(layer, k)
            if k == 0:
                part_ready(2 * layer)
            project(layer, k)
            tail_send(layer, k)
            if layer or k == 0:
                gh.drained()
        event3(o_now)
        if more:
            start_part(p_next)
        event4(o_now)
        for k in range(2):
            tail_recv(layer, k)
            convolve(layer, k)
            stats_send(k)
        gm = [mixed_gather(k) for k in range(2)]
        for k in range(2):
            mix(layer, k)
            stats_sent(k)
            gm[k].first()
        if more:
            event1(p_next)
        for k in range(2):
            gm[k].second()
        for k in range(2):
            gm[k].third()
        if more:
            event2(p_next)
        part_ready(o_now)
        for k in range(2):
            gm[k].last()
            contract(layer, k)
            gm[k].drained()
            if more:
                xg[k, :, lanes(me * ds_, ds_)] = state[k]
                hidden_gather(layer + 1, k).first()
        if more:
            event3(p_next)
            start_part(o_next)
            for k in range(2):
                hidden_gather(layer + 1, k).second()
            event4(p_next)
            for k in range(2):
                hidden_gather(layer + 1, k).third()

    half = final.at[:, lanes(h * ds_, ds_)]
    send(state.at[1 - ko], half, f_sem.at[1], f_sem.at[2], zpeer)
    final[:, lanes(h * ds_, ds_)] = state[ko]
    for layer in range(LAYERS):
        for k in range(2):
            tail_sent(layer, k)
    for q in range(parts):
        part_sent(q)
    send_wait(half, f_sem.at[1])
    recv_wait(final.at[:, lanes((1 - h) * ds_, ds_)], f_sem.at[2])
    done = pltpu.make_async_copy(final, out, f_sem.at[0])
    done.start()
    done.wait()


def per_device(
    sizes, hidden, doc_ids, norm_gain, w_value, w_gate, conv_taps, conv_bias, chan_gain, chan_bias, w_out
):
    SP, TP = sizes
    Z, Y = grid_of(SP)
    X = TP // 2
    T = hidden.shape[0]
    D = hidden.shape[1] * TP
    C = w_value.shape[2] * TP
    LAYERS, WIDTH = conv_taps.shape[0], conv_taps.shape[1]
    S = 4 * X
    cs, ds_ = C // S, D // S
    rp, ro = D // SP, C // SP
    bf, f32 = jnp.bfloat16, jnp.float32

    docs = lax.all_gather(doc_ids, "sp", tiled=True)
    spi = lax.axis_index("sp")
    z, y = spi // Y, spi % Y
    starts = jnp.stack([((z // 2) * 2 + k) * Y + y for k in range(2)]) * T
    where = starts[:, None] + jnp.arange(T)[None, :]
    mine = jnp.stack([lax.dynamic_slice_in_dim(docs, starts[k], T) for k in range(2)])
    before = jnp.sum((docs[None, None, :] < mine[:, :, None]).astype(jnp.int32), axis=-1)
    pos = jnp.broadcast_to((where - before)[:, :, None], (2, T, 128)).astype(jnp.int32)

    dims = (Z, Y, X, T, D, C, LAYERS, WIDTH)
    parts = 2 * LAYERS
    nx, ny = X - 1, Y - 1
    dma = pltpu.SemaphoreType.DMA
    vm = pl.BlockSpec(memory_space=pltpu.VMEM)
    hbm = pl.BlockSpec(memory_space=pl.ANY)
    return pl.pallas_call(
        functools.partial(kernel, dims),
        out_shape=jax.ShapeDtypeStruct((T, 2 * ds_), bf),
        in_specs=[hbm, vm, vm, hbm, hbm, vm, vm, vm, vm, hbm],
        out_specs=hbm,
        scratch_shapes=[
            pltpu.VMEM((LAYERS, SP, rp, 2 * cs), bf),
            pltpu.VMEM((LAYERS, SP, ro, ds_), bf),
            pltpu.VMEM((LAYERS, 3, rp, 2 * cs), bf),
            pltpu.VMEM((LAYERS, 3, ro, ds_), bf),
            pltpu.VMEM((2, T, D), bf),
            pltpu.VMEM((T, D), bf),
            pltpu.VMEM((2, T, C), bf),
            pltpu.VMEM((T, 2 * cs), f32),
            pltpu.VMEM((T, ds_), f32),
            pltpu.VMEM((2, T + HALO, cs), f32),
            pltpu.VMEM((2, T, cs), f32),
            pltpu.VMEM((2, T, ds_), bf),
            pltpu.VMEM((T, 2 * ds_), bf),
            pltpu.VMEM((LAYERS, 2, HALO, cs), bf),
            pltpu.VMEM((LAYERS, 2, HALO, cs), bf),
            pltpu.VMEM((T, 128), f32),
            pltpu.VMEM((2, 8, T), f32),
            pltpu.VMEM((2, S, 8, T), f32),
            pltpu.VMEM((2, T, 128), f32),
            dma((parts,)),
            dma((parts, 3)),
            dma((parts, 3)),
            dma((parts, Z, ny)),
            dma((parts, 7)),
            dma((parts, Z, ny)),
            dma((2, 3 + 4 * nx)),
            dma((2, 3 + 4 * nx)),
            dma((2, 3 + 4 * nx)),
            dma((2, 3 + 4 * nx)),
            dma((2, S)),
            dma((2, S)),
            dma((LAYERS, 2)),
            dma((LAYERS, 2)),
            dma((3,)),
        ],
        compiler_params=pltpu.CompilerParams(has_side_effects=True, vmem_limit_bytes=60 << 20),
        name="stack",
    )(hidden, pos, norm_gain, w_value, w_gate, conv_taps, conv_bias, chan_gain, chan_bias, w_out)


def solution(mesh):
    placed = (
        P("sp", "tp"),
        P("sp"),
        P(),
        P(None, "sp", "tp"),
        P(None, "sp", "tp"),
        P(None, None, "tp"),
        P(None, "tp"),
        P(None, "tp"),
        P(None, "tp"),
        P(None, "sp", "tp"),
    )
    sizes = (mesh.shape["sp"], mesh.shape["tp"])
    return jax.shard_map(
        functools.partial(per_device, sizes),
        mesh=mesh,
        in_specs=placed,
        out_specs=P("sp", "tp"),
        check_vma=False,
    )
```

```python
import functools
import math

import jax
import jax.numpy as jnp
from jax import lax
from jax.experimental import pallas as pl
from jax.experimental.pallas import tpu as pltpu
from jax.sharding import PartitionSpec as P

MESH = pl.DeviceIdType.MESH
HALO = 32
ROWS = 64


def grid_of(size):
    inner = max(d for d in range(1, math.isqrt(size) + 1) if size % d == 0)
    return size // inner, inner


def kernel(
    dims,
    hid,
    docs,
    ngain,
    wv,
    wg,
    taps,
    cbias,
    cgain,
    chbias,
    wo,
    out,
    wp_buf,
    wo_buf,
    rp_buf,
    ro_buf,
    xg,
    xn,
    mg,
    prod,
    branch,
    glu,
    conv,
    state,
    final,
    tail,
    halo,
    stat,
    stat_out,
    stat_in,
    cols,
    pos,
    doc_halo,
    loc_sem,
    z_recv,
    r_recv,
    y_recv,
    z_send,
    y_send,
    h_recv,
    h_send,
    m_recv,
    m_send,
    s_recv,
    s_send,
    t_recv,
    t_send,
    f_sem,
    d_sem,
):
    Z, Y, X, T, D, C, LAYERS, WIDTH = dims
    S = 4 * X
    cs, ds_ = C // S, D // S
    parts = 2 * LAYERS
    nx, ny = X - 1, Y - 1

    spi, tpi = lax.axis_index("sp"), lax.axis_index("tp")
    z, y, x, c = spi // Y, spi % Y, tpi // 2, tpi % 2
    zn = z + 1 - 2 * (z % 2)
    zh, ko = z // 2, z % 2
    inner = ((z + 1) // 2) % 2
    h = 1 - inner
    zin = inner * z + h * zn
    zout = h * z + inner * zn
    me = (x * 2 + c) * 2 + h

    def dev(zz, yy, xx, cc):
        return (zz * Y + yy, xx * 2 + cc)

    partner = dev(z, y, x, 1 - c)
    zpeer = dev(zn, y, x, c)
    mid = dev(Z - 1 - z, y, x, c)

    def send(src, dst, ssem, rsem, device):
        pltpu.make_async_remote_copy(
            src_ref=src, dst_ref=dst, send_sem=ssem, recv_sem=rsem,
            device_id=device, device_id_type=MESH,
        ).start()

    def recv_wait(ref, sem):
        pltpu.make_async_remote_copy(
            src_ref=ref, dst_ref=ref, send_sem=sem, recv_sem=sem,
            device_id=partner, device_id_type=MESH,
        ).wait_recv()

    def send_wait(ref, sem):
        pltpu.make_async_remote_copy(
            src_ref=ref, dst_ref=ref, send_sem=sem, recv_sem=sem,
            device_id=partner, device_id_type=MESH,
        ).wait_send()

    def lanes(start, size):
        return pl.ds(pl.multiple_of(start, 128), size)

    def block(q, b):
        return (wo_buf if q % 2 else wp_buf).at[q // 2, b]

    def relay(q, i):
        return (ro_buf if q % 2 else rp_buf).at[q // 2, i]

    def own_pieces(q, half, dst):
        l = q // 2
        if q % 2:
            return [(wo.at[l, :, lanes(half * ds_, ds_)], dst)]
        return [
            (wv.at[l, :, lanes(half * cs, cs)], dst.at[:, pl.ds(0, cs)]),
            (wg.at[l, :, lanes(half * cs, cs)], dst.at[:, pl.ds(cs, cs)]),
        ]

    def own_send(q, half, dst, ssem, rsem, device):
        for src, part in own_pieces(q, half, dst):
            send(src, part, ssem, rsem, device)

    def y_spread(q, zb):
        b = zb * Y + y
        for j in range(1, Y):
            send(block(q, b), block(q, b), y_send.at[q, zb, j - 1], y_recv.at[q, zb, j - 1],
                 dev(z, (y + j) % Y, x, c))

    def start_part(q):
        mine = block(q, z * Y + y)
        own_send(q, 1 - h, mine, z_send.at[q, 0], z_recv.at[q, 0], zpeer)

        @pl.when(inner == 0)
        def _():
            own_send(q, h, relay(q, 1), z_send.at[q, 1], r_recv.at[q, 1], zpeer)

        @pl.when(inner == 1)
        def _():
            own_send(q, 1 - h, relay(q, 0), z_send.at[q, 1], r_recv.at[q, 0], mid)
            own_send(q, h, mine, z_send.at[q, 2], z_recv.at[q, 1], mid)

        for j in range(1, Y):
            own_send(q, h, mine, y_send.at[q, z, j - 1], y_recv.at[q, z, j - 1],
                     dev(z, (y + j) % Y, x, c))
        for src, part in own_pieces(q, h, mine):
            pltpu.make_async_copy(src, part, loc_sem.at[q]).start()

    def event1(q):
        recv_wait(block(q, zn * Y + y), z_recv.at[q, 0])
        y_spread(q, zn)

    def relay1(q):
        @pl.when(inner == 1)
        def _():
            recv_wait(relay(q, 0), r_recv.at[q, 0])
            send(relay(q, 0), block(q, (Z - 1 - z) * Y + y), z_send.at[q, 3], z_recv.at[q, 1], zpeer)

    def event2(q):
        @pl.when(inner == 1)
        def _():
            recv_wait(relay(q, 1), r_recv.at[q, 1])
            send(relay(q, 1), relay(q, 2), z_send.at[q, 4], r_recv.at[q, 2], mid)
            near = block(q, zn * Y + y)
            send(near, near, z_send.at[q, 5], z_recv.at[q, 2], mid)

        zb = Z - 1 - zin
        recv_wait(block(q, zb * Y + y), z_recv.at[q, 1])
        y_spread(q, zb)

    def event3(q):
        @pl.when(inner == 1)
        def _():
            recv_wait(relay(q, 2), r_recv.at[q, 2])
            send(relay(q, 2), block(q, (Z - 1 - zn) * Y + y), z_send.at[q, 6], z_recv.at[q, 2], zpeer)

    def event4(q):
        zb = Z - 1 - zout
        recv_wait(block(q, zb * Y + y), z_recv.at[q, 2])
        y_spread(q, zb)

    def part_ready(q):
        mine = block(q, z * Y + y)
        pltpu.make_async_copy(mine, mine, loc_sem.at[q]).wait()
        for zb in range(Z):
            for j in range(1, Y):
                recv_wait(block(q, zb * Y + (y - j + Y) % Y), y_recv.at[q, zb, j - 1])

    def part_sent(q):
        ref = block(q, 0)
        for zb in range(Z):
            for j in range(1, Y):
                send_wait(ref, y_send.at[q, zb, j - 1])
        send_wait(ref, z_send.at[q, 0])
        send_wait(ref, z_send.at[q, 1])

        @pl.when(inner == 1)
        def _():
            for i in range(2, 7):
                send_wait(ref, z_send.at[q, i])

    class Gather:
        def __init__(self, region, recv, sent, source=None):
            self.region, self.recv, self.sent = region, recv, sent
            self.own = region(x, c, z)
            self.source = self.own if source is None else source

        def xs(self, j):
            return (x - j + X) % X

        def forward(self, ref, i, device):
            send(ref, ref, self.sent.at[i], self.recv.at[i], device)

        def first(self):
            def go(i, device):
                send(self.source, self.own, self.sent.at[i], self.recv.at[i], device)

            go(1, zpeer)
            for j in range(1, X):
                go(2 + j, dev(z, y, (x + j) % X, c))
            go(0, partner)

        def second(self):
            ref = self.region(x, c, zn)
            recv_wait(ref, self.recv.at[1])
            for j in range(1, X):
                self.forward(ref, 2 + nx + j, dev(z, y, (x + j) % X, c))
            self.forward(ref, 2, partner)

        def third(self):
            for j in range(1, X):
                ref = self.region(self.xs(j), c, z)
                recv_wait(ref, self.recv.at[2 + j])
                self.forward(ref, 2 + 2 * nx + j, partner)

        def fourth(self):
            for j in range(1, X):
                ref = self.region(self.xs(j), c, zn)
                recv_wait(ref, self.recv.at[2 + nx + j])
                self.forward(ref, 2 + 3 * nx + j, partner)

        def last(self):
            recv_wait(self.region(x, 1 - c, z), self.recv.at[0])
            recv_wait(self.region(x, 1 - c, zn), self.recv.at[2])
            for j in range(1, X):
                recv_wait(self.region(self.xs(j), 1 - c, z), self.recv.at[2 + 2 * nx + j])
                recv_wait(self.region(self.xs(j), 1 - c, zn), self.recv.at[2 + 3 * nx + j])

        def drained(self):
            for i in range(3 + 4 * nx):
                send_wait(self.own, self.sent.at[i])

    def slot(xx, cc, zz):
        return (xx * 2 + cc) * 2 + 1 - ((zz + 1) // 2) % 2

    def hidden_gather(layer, k):
        if layer == 0:
            return Gather(
                lambda xx, cc, zz: xg.at[zz % 2, :, lanes((xx * 2 + cc) * 2 * ds_, 2 * ds_)],
                h_recv.at[0], h_send.at[0], hid,
            )
        return Gather(
            lambda xx, cc, zz: xg.at[k, :, lanes(slot(xx, cc, zz) * ds_, ds_)],
            h_recv.at[k], h_send.at[k], state.at[k],
        )

    def mixed_gather(k):
        return Gather(
            lambda xx, cc, zz: mg.at[k, :, lanes(slot(xx, cc, zz) * cs, cs)],
            m_recv.at[k], m_send.at[k],
        )

    def normalise(layer, k):
        @pl.loop(0, T // 16, unroll=2)
        def _(i):
            rows = pl.ds(pl.multiple_of(i * 16, 16), 16)
            v = xg[k, rows, :].astype(jnp.float32)
            scale = lax.rsqrt(jnp.mean(v * v, axis=-1, keepdims=True) + 1e-6)
            cols[0, rows, :] = jnp.broadcast_to(scale, (16, 128))

        @pl.loop(0, T // 16)
        def _(i):
            rows = pl.ds(pl.multiple_of(i * 16, 16), 16)
            scale = cols[0, rows, :]
            for t in range(D // 128):
                at = slice(t * 128, (t + 1) * 128)
                v = xg[k, rows, at].astype(jnp.float32) * scale * ngain[layer : layer + 1, at]
                xn[rows, at] = v.astype(jnp.bfloat16)

    def matmul(acc, lhs, rhs, depth, count):
        acc[...] = jnp.zeros_like(acc)

        @pl.loop(0, count)
        def _(b):
            acc[...] += jnp.dot(
                lhs[:, lanes(b * depth, depth)], rhs[b], preferred_element_type=jnp.float32
            )

    def project(layer, k):
        matmul(prod, xn, wp_buf.at[layer], D // (Z * Y), Z * Y)

        @pl.loop(0, T // HALO)
        def _(i):
            rows = pl.ds(pl.multiple_of(i * HALO, HALO), HALO)
            v, g = prod[rows, 0:cs], prod[rows, cs : 2 * cs]
            r = (v * jax.nn.sigmoid(g)).astype(jnp.bfloat16)
            glu[k, pl.ds(pl.multiple_of(i * HALO + HALO, HALO), HALO), :] = r.astype(jnp.float32)

        tail[layer, k] = glu[k, T : T + HALO, :].astype(jnp.bfloat16)

    def tail_send(layer, k):
        def go(kk, device):
            send(tail.at[layer, k], halo.at[layer, kk], t_send.at[layer, k], t_recv.at[layer, kk], device)

        @pl.when(y < Y - 1)
        def _():
            go(k, dev(z, y + 1, x, c))

        if k == 0:
            @pl.when(y == Y - 1)
            def _():
                go(1, dev(z, 0, x, c))
        else:
            @pl.when((y == Y - 1) & (zh == 0))
            def _():
                go(0, dev(Z - 1 - z, 0, x, c))

    def tail_sent(layer, k):
        if k == 0:
            send_wait(tail.at[layer, k], t_send.at[layer, k])
        else:
            @pl.when((y < Y - 1) | (zh == 0))
            def _():
                send_wait(tail.at[layer, k], t_send.at[layer, k])

    def tail_recv(layer, k):
        def arrive():
            recv_wait(halo.at[layer, k], t_recv.at[layer, k])
            glu[k, 0:HALO, :] = halo[layer, k].astype(jnp.float32)

        if k == 1:
            arrive()
        else:
            @pl.when((y > 0) | (zh > 0))
            def _():
                arrive()

            @pl.when((y == 0) & (zh == 0))
            def _():
                glu[k, 0:HALO, :] = jnp.zeros((HALO, cs), jnp.float32)

    def convolve(layer, k):
        first_lane = lax.broadcasted_iota(jnp.int32, (ROWS, 128), 1) == 0

        @pl.loop(0, T // ROWS)
        def _(i):
            base = pl.multiple_of(i * ROWS, ROWS)
            near = pos[k, pl.ds(base, ROWS), :]
            total = jnp.zeros((ROWS, 128), jnp.float32)
            square = jnp.zeros((ROWS, 128), jnp.float32)
            for t in range(cs // 128):
                at = lanes(h * cs + t * 128, 128)
                span = glu[k, pl.ds(base, ROWS + HALO), t * 128 : (t + 1) * 128]
                acc = jnp.broadcast_to(cbias[layer : layer + 1, at], (ROWS, 128))
                for phase in range(8):
                    moved = span if phase == 0 else pltpu.roll(span, ROWS + HALO - phase, 0)
                    for off in range(phase, HALO + 1, 8):
                        index = off - (HALO - (WIDTH - 1))
                        if 0 <= index < WIDTH:
                            start = off - phase
                            term = moved[start : start + ROWS] * taps[layer, index : index + 1, at]
                            back = WIDTH - 1 - index
                            acc = acc + (jnp.where(near >= back, term, 0.0) if back else term)
                conv[k, pl.ds(base, ROWS), t * 128 : (t + 1) * 128] = acc
                total = total + acc
                square = square + acc * acc
            s1 = jnp.sum(total, axis=1, keepdims=True)
            s2 = jnp.sum(square, axis=1, keepdims=True)
            stat[pl.ds(base, ROWS), :] = jnp.where(first_lane, s1, s2)

        for t in range(T // 128):
            stat_out[k, :, t * 128 : (t + 1) * 128] = stat[t * 128 : (t + 1) * 128, :].T[0:8, :]

    def others():
        for xj in range(X):
            for cj in range(2):
                for zj in range(2):
                    if xj or cj or zj:
                        xx, cc = (x + xj) % X, (c + cj) % 2
                        zz, zb = (zn, zn) if zj else (z, z)
                        back = ((x - xj + X) % X, (c + cj) % 2, zz)
                        yield (xj * 2 + cj) * 2 + zj, dev(zz, y, xx, cc), slot(*back)

    def stats_send(k):
        for i, device, _ in others():
            send(stat_out.at[k], stat_in.at[k, me], s_send.at[k, i], s_recv.at[k, i], device)

    def mix(layer, k):
        for i, _, theirs in others():
            recv_wait(stat_in.at[k, theirs], s_recv.at[k, i])
        stat_in[k, me] = stat_out[k]
        total = stat_in[k, 0]
        for i in range(1, S):
            total = total + stat_in[k, i]
        for t in range(T // 128):
            tile = total[:, t * 128 : (t + 1) * 128]
            turned = jnp.concatenate([tile] * 16, axis=0).T
            mu = turned[:, 0:1] * (1.0 / C)
            var = turned[:, 1:2] * (1.0 / C) - mu * mu
            rows = slice(t * 128, (t + 1) * 128)
            cols[0, rows, :] = jnp.broadcast_to(mu, (128, 128))
            cols[1, rows, :] = jnp.broadcast_to(lax.rsqrt(var + 1e-5), (128, 128))

        @pl.loop(0, T // ROWS)
        def _(i):
            rows = pl.ds(pl.multiple_of(i * ROWS, ROWS), ROWS)
            mu, scale = cols[0, rows, :], cols[1, rows, :]
            for t in range(cs // 128):
                at = lanes(h * cs + t * 128, 128)
                v = (conv[k, rows, t * 128 : (t + 1) * 128] - mu) * scale
                v = v * cgain[layer : layer + 1, at] + chbias[layer : layer + 1, at]
                mg[k, rows, lanes(me * cs + t * 128, 128)] = jax.nn.silu(v).astype(jnp.bfloat16)

    def stats_sent(k):
        for i, _, _ in others():
            send_wait(stat_out.at[k], s_send.at[k, i])

    def contract(layer, k):
        matmul(branch, mg.at[k], wo_buf.at[layer], C // (Z * Y), Z * Y)
        state[k] = (state[k].astype(jnp.float32) + branch[...]).astype(jnp.bfloat16)

    def docs_start():
        tail_docs = docs.at[pl.ds(T - HALO, HALO)]

        @pl.when(y < Y - 1)
        def _():
            send(tail_docs, doc_halo, d_sem.at[0], d_sem.at[1], dev(z, y + 1, x, c))

        @pl.when((y == Y - 1) & (z < Z - 1))
        def _():
            send(tail_docs, doc_halo, d_sem.at[0], d_sem.at[1], dev(z + 1, 0, x, c))

    def docs_done():
        @pl.when((y > 0) | (z > 0))
        def _():
            recv_wait(doc_halo, d_sem.at[1])

        @pl.when((y == 0) & (z == 0))
        def _():
            doc_halo[...] = jnp.full((HALO, 128), -1, jnp.int32)

        def count(base, span):
            here = span[HALO:]
            total = jnp.zeros((ROWS, 128), jnp.int32)
            for phase in range(8):
                moved = span if phase == 0 else pltpu.roll(span, ROWS + HALO - phase, 0)
                for off in range(phase, HALO, 8):
                    if off >= HALO - (WIDTH - 1):
                        start = off - phase
                        same = moved[start : start + ROWS] == here
                        total = total + jnp.where(same, 1, 0)
            pos[ko, pl.ds(base, ROWS), :] = total

        count(0, jnp.concatenate([doc_halo[...], docs[0:ROWS, :]], axis=0))

        @pl.loop(1, T // ROWS)
        def _(i):
            base = pl.multiple_of(i * ROWS, ROWS)
            count(base, docs[pl.ds(pl.multiple_of(base - HALO, HALO), ROWS + HALO), :])

        send(pos.at[ko], pos.at[ko], d_sem.at[2], d_sem.at[3], zpeer)

    def docs_sent():
        @pl.when((y < Y - 1) | (z < Z - 1))
        def _():
            send_wait(doc_halo, d_sem.at[0])

        send_wait(pos.at[ko], d_sem.at[2])

    own0 = xg.at[ko, :, lanes((x * 2 + c) * 2 * ds_, 2 * ds_)]
    local = pltpu.make_async_copy(hid, own0, f_sem.at[0])
    local.start()
    docs_start()
    start_part(0)
    gh = [hidden_gather(0, 0)]
    gh[0].first()
    docs_done()
    event1(0)
    relay1(0)
    event2(0)
    start_part(1)
    gh[0].second()
    event3(0)
    gh[0].third()
    local.wait()
    event4(0)

    for layer in range(LAYERS):
        p_now, o_now, p_next = 2 * layer, 2 * layer + 1, 2 * layer + 2
        more = layer + 1 < LAYERS
        if layer:
            event3(p_now)
            gh[0].second()
            gh[0].third()
            start_part(o_now)
            event4(p_now)
            gh[1].second()
            gh[1].third()
        event1(o_now)
        relay1(o_now)
        event2(o_now)
        for k in range(2):
            if k < len(gh):
                gh[k].fourth()
                gh[k].last()
            if layer == 0 and k == 0:
                for kk in range(2):
                    state[kk] = xg[kk, :, lanes(me * ds_, ds_)]
            normalise(layer, k)
            if k == 0:
                part_ready(p_now)
            project(layer, k)
            tail_send(layer, k)
            if k < len(gh):
                gh[k].drained()
            if k == 0:
                event3(o_now)
                if more:
                    start_part(p_next)
        event4(o_now)
        if layer == 0:
            recv_wait(pos.at[1 - ko], d_sem.at[3])
        for k in range(2):
            tail_recv(layer, k)
            if layer:
                stats_sent(k)
            convolve(layer, k)
            stats_send(k)
        if more:
            event1(p_next)
        gm = [mixed_gather(k) for k in range(2)]
        for k in range(2):
            mix(layer, k)
            gm[k].first()
        if more:
            relay1(p_next)
        for k in range(2):
            gm[k].second()
            gm[k].third()
        if more:
            event2(p_next)
        for k in range(2):
            gm[k].fourth()
            gm[k].last()
            if k == 0:
                part_ready(o_now)
            contract(layer, k)
            gm[k].drained()
            if more:
                xg[k, :, lanes(me * ds_, ds_)] = state[k]
                if k == 0:
                    gh = [hidden_gather(layer + 1, kk) for kk in range(2)]
                gh[k].first()

    for k in range(2):
        stats_sent(k)
    docs_sent()
    half = final.at[:, lanes(h * ds_, ds_)]
    send(state.at[1 - ko], half, f_sem.at[1], f_sem.at[2], zpeer)
    final[:, lanes(h * ds_, ds_)] = state[ko]
    for layer in range(LAYERS):
        for k in range(2):
            tail_sent(layer, k)
    for q in range(parts):
        part_sent(q)
    send_wait(half, f_sem.at[1])
    recv_wait(final.at[:, lanes((1 - h) * ds_, ds_)], f_sem.at[2])
    done = pltpu.make_async_copy(final, out, f_sem.at[0])
    done.start()
    done.wait()


def per_device(
    sizes, hidden, doc_ids, norm_gain, w_value, w_gate, conv_taps, conv_bias, chan_gain, chan_bias, w_out
):
    SP, TP = sizes
    Z, Y = grid_of(SP)
    X = TP // 2
    T = hidden.shape[0]
    D = hidden.shape[1] * TP
    C = w_value.shape[2] * TP
    LAYERS, WIDTH = conv_taps.shape[0], conv_taps.shape[1]
    S = 4 * X
    cs, ds_ = C // S, D // S
    rp, ro = D // SP, C // SP
    bf, f32 = jnp.bfloat16, jnp.float32

    docs = jnp.broadcast_to(doc_ids[:, None], (T, 128))

    dims = (Z, Y, X, T, D, C, LAYERS, WIDTH)
    parts = 2 * LAYERS
    nx, ny = X - 1, Y - 1
    dma = pltpu.SemaphoreType.DMA
    vm = pl.BlockSpec(memory_space=pltpu.VMEM)
    hbm = pl.BlockSpec(memory_space=pl.ANY)
    return pl.pallas_call(
        functools.partial(kernel, dims),
        out_shape=jax.ShapeDtypeStruct((T, 2 * ds_), bf),
        in_specs=[hbm, vm, vm, hbm, hbm, vm, vm, vm, vm, hbm],
        out_specs=hbm,
        scratch_shapes=[
            pltpu.VMEM((LAYERS, SP, rp, 2 * cs), bf),
            pltpu.VMEM((LAYERS, SP, ro, ds_), bf),
            pltpu.VMEM((LAYERS, 3, rp, 2 * cs), bf),
            pltpu.VMEM((LAYERS, 3, ro, ds_), bf),
            pltpu.VMEM((2, T, D), bf),
            pltpu.VMEM((T, D), bf),
            pltpu.VMEM((2, T, C), bf),
            pltpu.VMEM((T, 2 * cs), f32),
            pltpu.VMEM((T, ds_), f32),
            pltpu.VMEM((2, T + HALO, cs), f32),
            pltpu.VMEM((2, T, cs), f32),
            pltpu.VMEM((2, T, ds_), bf),
            pltpu.VMEM((T, 2 * ds_), bf),
            pltpu.VMEM((LAYERS, 2, HALO, cs), bf),
            pltpu.VMEM((LAYERS, 2, HALO, cs), bf),
            pltpu.VMEM((T, 128), f32),
            pltpu.VMEM((2, 8, T), f32),
            pltpu.VMEM((2, S, 8, T), f32),
            pltpu.VMEM((2, T, 128), f32),
            pltpu.VMEM((2, T, 128), jnp.int32),
            pltpu.VMEM((HALO, 128), jnp.int32),
            dma((parts,)),
            dma((parts, 3)),
            dma((parts, 3)),
            dma((parts, Z, ny)),
            dma((parts, 7)),
            dma((parts, Z, ny)),
            dma((2, 3 + 4 * nx)),
            dma((2, 3 + 4 * nx)),
            dma((2, 3 + 4 * nx)),
            dma((2, 3 + 4 * nx)),
            dma((2, S)),
            dma((2, S)),
            dma((LAYERS, 2)),
            dma((LAYERS, 2)),
            dma((3,)),
            dma((4,)),
        ],
        compiler_params=pltpu.CompilerParams(has_side_effects=True, vmem_limit_bytes=60 << 20),
        name="stack",
    )(hidden, docs, norm_gain, w_value, w_gate, conv_taps, conv_bias, chan_gain, chan_bias, w_out)


def solution(mesh):
    placed = (
        P("sp", "tp"),
        P("sp"),
        P(),
        P(None, "sp", "tp"),
        P(None, "sp", "tp"),
        P(None, None, "tp"),
        P(None, "tp"),
        P(None, "tp"),
        P(None, "tp"),
        P(None, "sp", "tp"),
    )
    sizes = (mesh.shape["sp"], mesh.shape["tp"])
    return jax.shard_map(
        functools.partial(per_device, sizes),
        mesh=mesh,
        in_specs=placed,
        out_specs=P("sp", "tp"),
        check_vma=False,
    )
```

```python
import functools
import math

import jax
import jax.numpy as jnp
from jax import lax
from jax.experimental import pallas as pl
from jax.experimental.pallas import tpu as pltpu
from jax.sharding import PartitionSpec as P

MESH = pl.DeviceIdType.MESH
HALO = 32
ROWS = 64


def grid_of(size):
    inner = max(d for d in range(1, math.isqrt(size) + 1) if size % d == 0)
    return size // inner, inner


def kernel(
    dims,
    hid,
    docs,
    ngain,
    wv,
    wg,
    taps,
    cbias,
    cgain,
    chbias,
    wo,
    out,
    wp_buf,
    wo_buf,
    stage_p,
    stage_o,
    xg,
    xn,
    mg,
    prod,
    branch,
    glu,
    conv,
    state,
    final,
    tail,
    halo,
    stat,
    stat_out,
    stat_in,
    stat_row,
    tail_relay,
    cols,
    pos,
    doc_halo,
    loc_sem,
    g_recv,
    g_send,
    z_recv,
    y_recv,
    z_send,
    y_send,
    h_recv,
    h_send,
    m_recv,
    m_send,
    s_recv,
    s_send,
    r_recv,
    r_send,
    k_recv,
    k_send,
    t_recv,
    t_send,
    f_sem,
    d_sem,
):
    Z, Y, X, T, D, C, LAYERS, WIDTH = dims
    S = 4 * X
    cs, ds_ = C // S, D // S
    parts = 2 * LAYERS
    nx, ny = X - 1, Y - 1

    spi, tpi = lax.axis_index("sp"), lax.axis_index("tp")
    z, y, x, c = spi // Y, spi % Y, tpi // 2, tpi % 2
    zn = z + 1 - 2 * (z % 2)
    zh, ko = z // 2, z % 2
    inner = ((z + 1) // 2) % 2
    h = 1 - inner
    zin = inner * z + h * zn
    zout = h * z + inner * zn
    me = (x * 2 + c) * 2 + h

    def dev(zz, yy, xx, cc):
        return (zz * Y + yy, xx * 2 + cc)

    partner = dev(z, y, x, 1 - c)
    zpeer = dev(zn, y, x, c)

    def send(src, dst, ssem, rsem, device):
        pltpu.make_async_remote_copy(
            src_ref=src, dst_ref=dst, send_sem=ssem, recv_sem=rsem,
            device_id=device, device_id_type=MESH,
        ).start()

    def recv_wait(ref, sem):
        pltpu.make_async_remote_copy(
            src_ref=ref, dst_ref=ref, send_sem=sem, recv_sem=sem,
            device_id=partner, device_id_type=MESH,
        ).wait_recv()

    def send_wait(ref, sem):
        pltpu.make_async_remote_copy(
            src_ref=ref, dst_ref=ref, send_sem=sem, recv_sem=sem,
            device_id=partner, device_id_type=MESH,
        ).wait_send()

    def lanes(start, size):
        return pl.ds(pl.multiple_of(start, 128), size)

    def block(q, b):
        return (wo_buf if q % 2 else wp_buf).at[q // 2, b]

    def own_pieces(q, half, dst, staged=False):
        l = q // 2
        if q % 2:
            src = stage_o if staged else wo
            return [(src.at[l, :, lanes(half * ds_, ds_)], dst)]
        low, high = dst.at[:, pl.ds(0, cs)], dst.at[:, pl.ds(cs, cs)]
        if staged:
            return [
                (stage_p.at[l, :, lanes(half * cs, cs)], low),
                (stage_p.at[l, :, lanes((half + 2) * cs, cs)], high),
            ]
        return [
            (wv.at[l, :, lanes(half * cs, cs)], low),
            (wg.at[l, :, lanes(half * cs, cs)], high),
        ]

    def own_send(q, half, dst, ssem, rsem, device, staged=False):
        for src, part in own_pieces(q, half, dst, staged):
            send(src, part, ssem, rsem, device)

    def hand_over(q):
        l = q // 2
        if q % 2:
            moves = [(wo.at[l], stage_o.at[l])]
        else:
            moves = [
                (wv.at[l], stage_p.at[l, :, pl.ds(0, 2 * cs)]),
                (wg.at[l], stage_p.at[l, :, pl.ds(2 * cs, 2 * cs)]),
            ]
        for src, dst in moves:
            send(src, dst, g_send.at[q], g_recv.at[q], partner)

    def staged_ref(q):
        return (stage_o if q % 2 else stage_p).at[q // 2]

    def z_sends(q):
        mine = block(q, z * Y + y)
        moves = [
            (1 - h, z_recv.at[q, 0], zn),
            (h, z_recv.at[q, 1 + h], Z - 1 - z),
            (1 - h, z_recv.at[q, 1 + h], Z - 1 - zn),
        ]
        for i, (half, rsem, zz) in enumerate(moves):
            for cc in (1, 0):
                if i == 0 and cc == 0:
                    recv_wait(staged_ref(q), g_recv.at[q])
                own_send(q, half, mine, z_send.at[q, cc, i], rsem, dev(zz, y, x, cc), cc == 0)

    def z_start(*qs, kind=None):
        @pl.when((c == 1) if kind is None else (c == 1) & (inner == kind))
        def _():
            for q in qs:
                z_sends(q)

    def y_spread(q, zb):
        b = zb * Y + y
        for j in range(1, Y):
            send(block(q, b), block(q, b), y_send.at[q, zb, j - 1], y_recv.at[q, zb, j - 1],
                 dev(z, (y + j) % Y, x, c))

    def start_part(q):
        mine = block(q, z * Y + y)
        for j in range(1, Y):
            own_send(q, h, mine, y_send.at[q, z, j - 1], y_recv.at[q, z, j - 1],
                     dev(z, (y + j) % Y, x, c))
        for src, part in own_pieces(q, h, mine):
            pltpu.make_async_copy(src, part, loc_sem.at[q]).start()

    def event1(q):
        recv_wait(block(q, zn * Y + y), z_recv.at[q, 0])
        y_spread(q, zn)

    def event2(q):
        zb = Z - 1 - zin
        recv_wait(block(q, zb * Y + y), z_recv.at[q, 1])
        y_spread(q, zb)

    def event3(q):
        zb = Z - 1 - zout
        recv_wait(block(q, zb * Y + y), z_recv.at[q, 2])
        y_spread(q, zb)

    def part_ready(q):
        mine = block(q, z * Y + y)
        pltpu.make_async_copy(mine, mine, loc_sem.at[q]).wait()
        for zb in range(Z):
            for j in range(1, Y):
                recv_wait(block(q, zb * Y + (y - j + Y) % Y), y_recv.at[q, zb, j - 1])

    def part_sent(q):
        ref = block(q, 0)
        for zb in range(Z):
            for j in range(1, Y):
                send_wait(ref, y_send.at[q, zb, j - 1])

        @pl.when(c == 1)
        def _():
            for cc in range(2):
                for i in range(3):
                    send_wait(ref, z_send.at[q, cc, i])

        @pl.when(c == 0)
        def _():
            send_wait(staged_ref(q), g_send.at[q])

    class Gather:
        def __init__(self, region, recv, sent, source=None):
            self.region, self.recv, self.sent = region, recv, sent
            self.own = region(x, c, z)
            self.source = self.own if source is None else source

        def xs(self, j):
            return (x - j + X) % X

        def forward(self, ref, i, device):
            send(ref, ref, self.sent.at[i], self.recv.at[i], device)

        def first(self):
            def go(i, device):
                send(self.source, self.own, self.sent.at[i], self.recv.at[i], device)

            for j in range(1, X):
                go(2 + j, dev(z, y, (x + j) % X, c))
            go(0, partner)

            @pl.when(c == 0)
            def _():
                go(1, zpeer)

        def across(self):
            @pl.when(c == 0)
            def _():
                ref = self.region(x, 1, z)
                recv_wait(ref, self.recv.at[0])
                send(ref, ref, self.sent.at[3 + 4 * nx], self.recv.at[1], dev(zn, y, x, 1))

        def second(self):
            ref = self.region(x, c, zn)
            recv_wait(ref, self.recv.at[1])
            for j in range(1, X):
                self.forward(ref, 2 + nx + j, dev(z, y, (x + j) % X, c))
            self.forward(ref, 2, partner)

        def third(self):
            for j in range(1, X):
                ref = self.region(self.xs(j), c, z)
                recv_wait(ref, self.recv.at[2 + j])
                self.forward(ref, 2 + 2 * nx + j, partner)

        def fourth(self):
            for j in range(1, X):
                ref = self.region(self.xs(j), c, zn)
                recv_wait(ref, self.recv.at[2 + nx + j])
                self.forward(ref, 2 + 3 * nx + j, partner)

        def last(self):
            @pl.when(c == 1)
            def _():
                recv_wait(self.region(x, 0, z), self.recv.at[0])

            recv_wait(self.region(x, 1 - c, zn), self.recv.at[2])
            for j in range(1, X):
                recv_wait(self.region(self.xs(j), 1 - c, z), self.recv.at[2 + 2 * nx + j])
                recv_wait(self.region(self.xs(j), 1 - c, zn), self.recv.at[2 + 3 * nx + j])

        def drained(self):
            for i in [0] + list(range(2, 3 + 4 * nx)):
                send_wait(self.own, self.sent.at[i])

            @pl.when(c == 0)
            def _():
                send_wait(self.own, self.sent.at[1])
                send_wait(self.own, self.sent.at[3 + 4 * nx])

    def slot(xx, cc, zz):
        return (xx * 2 + cc) * 2 + 1 - ((zz + 1) // 2) % 2

    def hidden_gather(layer, k):
        if layer == 0:
            return Gather(
                lambda xx, cc, zz: xg.at[zz % 2, :, lanes((xx * 2 + cc) * 2 * ds_, 2 * ds_)],
                h_recv.at[0], h_send.at[0], hid,
            )
        return Gather(
            lambda xx, cc, zz: xg.at[k, :, lanes(slot(xx, cc, zz) * ds_, ds_)],
            h_recv.at[k], h_send.at[k], state.at[k],
        )

    def mixed_gather(k):
        return Gather(
            lambda xx, cc, zz: mg.at[k, :, lanes(slot(xx, cc, zz) * cs, cs)],
            m_recv.at[k], m_send.at[k],
        )

    def normalise(layer, k):
        @pl.loop(0, T // 16, unroll=2)
        def _(i):
            rows = pl.ds(pl.multiple_of(i * 16, 16), 16)
            v = xg[k, rows, :].astype(jnp.float32)
            scale = lax.rsqrt(jnp.mean(v * v, axis=-1, keepdims=True) + 1e-6)
            cols[0, rows, :] = jnp.broadcast_to(scale, (16, 128))

        @pl.loop(0, T // 16)
        def _(i):
            rows = pl.ds(pl.multiple_of(i * 16, 16), 16)
            scale = cols[0, rows, :]
            for t in range(D // 128):
                at = slice(t * 128, (t + 1) * 128)
                v = xg[k, rows, at].astype(jnp.float32) * scale * ngain[layer : layer + 1, at]
                xn[rows, at] = v.astype(jnp.bfloat16)

    def matmul(acc, lhs, rhs, depth, count):
        acc[...] = jnp.zeros_like(acc)

        @pl.loop(0, count)
        def _(b):
            acc[...] += jnp.dot(
                lhs[:, lanes(b * depth, depth)], rhs[b], preferred_element_type=jnp.float32
            )

    def project(layer, k):
        matmul(prod, xn, wp_buf.at[layer], D // (Z * Y), Z * Y)

        @pl.loop(0, T // HALO)
        def _(i):
            rows = pl.ds(pl.multiple_of(i * HALO, HALO), HALO)
            v, g = prod[rows, 0:cs], prod[rows, cs : 2 * cs]
            r = (v * jax.nn.sigmoid(g)).astype(jnp.bfloat16)
            glu[k, pl.ds(pl.multiple_of(i * HALO + HALO, HALO), HALO), :] = r.astype(jnp.float32)

    def project_tail(layer, k):
        rows = slice(T - HALO, T)

        def step(b, acc):
            lhs = xn[rows, lanes(b * (D // (Z * Y)), D // (Z * Y))]
            return acc + jnp.dot(lhs, wp_buf[layer, b], preferred_element_type=jnp.float32)

        both = lax.fori_loop(0, Z * Y, step, jnp.zeros((HALO, 2 * cs), jnp.float32))
        tail[layer, k] = (both[:, 0:cs] * jax.nn.sigmoid(both[:, cs:])).astype(jnp.bfloat16)

    def tail_send(layer, k):
        def go(kk, device):
            send(tail.at[layer, k], halo.at[layer, kk], t_send.at[layer, k], t_recv.at[layer, kk], device)

        @pl.when(y < Y - 1)
        def _():
            go(k, dev(z, y + 1, x, c))

        if k == 0:
            @pl.when(y == Y - 1)
            def _():
                go(1, dev(z, 0, x, c))
        else:
            @pl.when((y == Y - 1) & (zh == 0) & (c == 0))
            def _():
                go(0, dev(Z - 1 - z, 0, x, 0))
                recv_wait(tail_relay.at[layer], k_recv.at[layer])
                send(tail_relay.at[layer], halo.at[layer, 0], k_send.at[layer], t_recv.at[layer, 0],
                     dev(Z - 1 - z, 0, x, 1))

            @pl.when((y == Y - 1) & (zh == 0) & (c == 1))
            def _():
                send(tail.at[layer, k], tail_relay.at[layer], t_send.at[layer, k], k_recv.at[layer], partner)

    def tail_sent(layer, k):
        if k == 0:
            send_wait(tail.at[layer, k], t_send.at[layer, k])
        else:
            @pl.when((y < Y - 1) | (zh == 0))
            def _():
                send_wait(tail.at[layer, k], t_send.at[layer, k])

            @pl.when((y == Y - 1) & (zh == 0) & (c == 0))
            def _():
                send_wait(tail_relay.at[layer], k_send.at[layer])

    def tail_recv(layer, k):
        def arrive():
            recv_wait(halo.at[layer, k], t_recv.at[layer, k])
            glu[k, 0:HALO, :] = halo[layer, k].astype(jnp.float32)

        if k == 1:
            arrive()
        else:
            @pl.when((y > 0) | (zh > 0))
            def _():
                arrive()

            @pl.when((y == 0) & (zh == 0))
            def _():
                glu[k, 0:HALO, :] = jnp.zeros((HALO, cs), jnp.float32)

    def convolve_tile(layer, k, base):
        first_lane = lax.broadcasted_iota(jnp.int32, (ROWS, 128), 1) == 0
        near = pos[k, pl.ds(base, ROWS), :]
        total = jnp.zeros((ROWS, 128), jnp.float32)
        square = jnp.zeros((ROWS, 128), jnp.float32)
        for t in range(cs // 128):
            at = lanes(h * cs + t * 128, 128)
            span = glu[k, pl.ds(base, ROWS + HALO), t * 128 : (t + 1) * 128]
            acc = jnp.broadcast_to(cbias[layer : layer + 1, at], (ROWS, 128))
            for phase in range(8):
                moved = span if phase == 0 else pltpu.roll(span, ROWS + HALO - phase, 0)
                for off in range(phase, HALO + 1, 8):
                    index = off - (HALO - (WIDTH - 1))
                    if 0 <= index < WIDTH:
                        start = off - phase
                        term = moved[start : start + ROWS] * taps[layer, index : index + 1, at]
                        back = WIDTH - 1 - index
                        acc = acc + (jnp.where(near >= back, term, 0.0) if back else term)
            conv[k, pl.ds(base, ROWS), t * 128 : (t + 1) * 128] = acc
            total = total + acc
            square = square + acc * acc
        s1 = jnp.sum(total, axis=1, keepdims=True)
        s2 = jnp.sum(square, axis=1, keepdims=True)
        stat[k, pl.ds(base, ROWS), :] = jnp.where(first_lane, s1, s2)

    def convolve(layer, k):
        @pl.loop(1, T // ROWS)
        def _(i):
            convolve_tile(layer, k, pl.multiple_of(i * ROWS, ROWS))

    def convolve_first(layer, k):
        convolve_tile(layer, k, 0)
        for t in range(T // 128):
            stat_out[k, :, t * 128 : (t + 1) * 128] = stat[k, t * 128 : (t + 1) * 128, :].T[0:8, :]

    def others():
        for xj in range(X):
            for cj in range(2):
                if xj or cj:
                    device = dev(z, y, (x + xj) % X, (c + cj) % 2)
                    yield xj * 2 + cj, device, (x - xj + X) % X * 2 + (c + cj) % 2

    def stats_send(k):
        for i, device, _ in others():
            send(stat_out.at[k], stat_in.at[k, x * 2 + c], s_send.at[k, i], s_recv.at[k, i], device)

    def row_sum(k):
        for i, _, theirs in others():
            recv_wait(stat_in.at[k, theirs], s_recv.at[k, i])
        stat_in[k, x * 2 + c] = stat_out[k]
        total = stat_in[k, 0]
        for i in range(1, 2 * X):
            total = total + stat_in[k, i]
        stat_row[k, h] = total

        @pl.when(c == 0)
        def _():
            for cc in range(2):
                send(stat_row.at[k, h], stat_row.at[k, h], r_send.at[k, cc], r_recv.at[k], dev(zn, y, x, cc))

    def mix(layer, k):
        recv_wait(stat_row.at[k, 1 - h], r_recv.at[k])
        total = stat_row[k, 0] + stat_row[k, 1]
        for t in range(T // 128):
            tile = total[:, t * 128 : (t + 1) * 128]
            turned = jnp.concatenate([tile] * 16, axis=0).T
            mu = turned[:, 0:1] * (1.0 / C)
            var = turned[:, 1:2] * (1.0 / C) - mu * mu
            rows = slice(t * 128, (t + 1) * 128)
            cols[0, rows, :] = jnp.broadcast_to(mu, (128, 128))
            cols[1, rows, :] = jnp.broadcast_to(lax.rsqrt(var + 1e-5), (128, 128))

        @pl.loop(0, T // ROWS)
        def _(i):
            rows = pl.ds(pl.multiple_of(i * ROWS, ROWS), ROWS)
            mu, scale = cols[0, rows, :], cols[1, rows, :]
            for t in range(cs // 128):
                at = lanes(h * cs + t * 128, 128)
                v = (conv[k, rows, t * 128 : (t + 1) * 128] - mu) * scale
                v = v * cgain[layer : layer + 1, at] + chbias[layer : layer + 1, at]
                mg[k, rows, lanes(me * cs + t * 128, 128)] = jax.nn.silu(v).astype(jnp.bfloat16)

    def stats_sent(k):
        for i, _, _ in others():
            send_wait(stat_out.at[k], s_send.at[k, i])

        @pl.when(c == 0)
        def _():
            for cc in range(2):
                send_wait(stat_row.at[k, h], r_send.at[k, cc])

    def contract(layer, k):
        matmul(branch, mg.at[k], wo_buf.at[layer], C // (Z * Y), Z * Y)
        state[k] = (state[k].astype(jnp.float32) + branch[...]).astype(jnp.bfloat16)

    def docs_start():
        tail_docs = docs.at[pl.ds(T - HALO, HALO)]

        @pl.when(y < Y - 1)
        def _():
            send(tail_docs, doc_halo, d_sem.at[0], d_sem.at[1], dev(z, y + 1, x, c))

        @pl.when((y == Y - 1) & (z < Z - 1))
        def _():
            send(tail_docs, doc_halo, d_sem.at[0], d_sem.at[1], dev(z + 1, 0, x, c))

    def docs_done():
        @pl.when((y > 0) | (z > 0))
        def _():
            recv_wait(doc_halo, d_sem.at[1])

        @pl.when((y == 0) & (z == 0))
        def _():
            doc_halo[...] = jnp.full((HALO, 128), -1, jnp.int32)

        def count(base, span):
            here = span[HALO:]
            total = jnp.zeros((ROWS, 128), jnp.int32)
            for phase in range(8):
                moved = span if phase == 0 else pltpu.roll(span, ROWS + HALO - phase, 0)
                for off in range(phase, HALO, 8):
                    if off >= HALO - (WIDTH - 1):
                        start = off - phase
                        same = moved[start : start + ROWS] == here
                        total = total + jnp.where(same, 1, 0)
            pos[ko, pl.ds(base, ROWS), :] = total

        count(0, jnp.concatenate([doc_halo[...], docs[0:ROWS, :]], axis=0))

        @pl.loop(1, T // ROWS)
        def _(i):
            base = pl.multiple_of(i * ROWS, ROWS)
            count(base, docs[pl.ds(pl.multiple_of(base - HALO, HALO), ROWS + HALO), :])

        @pl.when(c == 0)
        def _():
            send(pos.at[ko], pos.at[ko], d_sem.at[2], d_sem.at[3], dev(zn, y, x, 0))
            send(pos.at[ko], pos.at[ko], d_sem.at[4], d_sem.at[3], dev(zn, y, x, 1))

    def docs_sent():
        @pl.when((y < Y - 1) | (z < Z - 1))
        def _():
            send_wait(doc_halo, d_sem.at[0])

        @pl.when(c == 0)
        def _():
            send_wait(pos.at[ko], d_sem.at[2])
            send_wait(pos.at[ko], d_sem.at[4])

    own0 = xg.at[ko, :, lanes((x * 2 + c) * 2 * ds_, 2 * ds_)]
    local = pltpu.make_async_copy(hid, own0, f_sem.at[0])
    local.start()
    docs_start()

    @pl.when(c == 0)
    def _():
        for q in range(parts):
            hand_over(q)

    start_part(0)

    z_start(0)

    gh = [hidden_gather(0, 0)]
    gh[0].first()
    gh[0].across()
    docs_done()
    event1(0)
    event2(0)
    gh[0].third()
    gh[0].second()
    local.wait()
    z_start(1, 2, kind=0)
    event3(0)
    z_start(1, 2, kind=1)
    start_part(1)

    gm = None
    for layer in range(LAYERS):
        p_now, o_now, p_next = 2 * layer, 2 * layer + 1, 2 * layer + 2
        more = layer + 1 < LAYERS

        def mixed_out(k):
            gm[k].fourth()
            gm[k].last()
            if k == 0:
                part_ready(o_now)
            contract(layer, k)
            if more:
                xg[k, :, lanes(me * ds_, ds_)] = state[k]
                gather = hidden_gather(layer + 1, k)
                gather.first()
                gather.across()
                return gather

        if layer:
            gh[0].second()
            gh[0].third()
            event2(p_now)
            event3(p_now)
            start_part(o_now)
            gh[1].third()
            gh[1].second()
            z_start(*([o_now, p_next] if more else [o_now]))
        for k in range(2):
            if k < len(gh):
                gh[k].fourth()
                gh[k].last()
            if layer == 0 and k == 0:
                for kk in range(2):
                    state[kk] = xg[kk, :, lanes(me * ds_, ds_)]
            normalise(layer, k)
            if k == 0:
                part_ready(p_now)
            project_tail(layer, k)
            tail_send(layer, k)
            project(layer, k)
            if k < len(gh):
                gh[k].drained()
            if k == 0:
                if layer == 0:
                    recv_wait(pos.at[1 - ko], d_sem.at[3])
                else:
                    stats_sent(0)
                    stats_sent(1)
            convolve(layer, k)
            if k == 0:
                event1(o_now)
                event2(o_now)
        for k in range(2):
            tail_recv(layer, k)
            convolve_first(layer, k)
            if layer:
                gm[k].drained()
            stats_send(k)
        event3(o_now)
        if more:
            start_part(p_next)
        for k in range(2):
            row_sum(k)
        gm = [mixed_gather(k) for k in range(2)]
        for k in range(2):
            mix(layer, k)
            gm[k].first()
            gm[k].across()
        if more:
            event1(p_next)
        gm[0].third()
        gm[0].second()
        gm[1].third()
        gm[1].second()
        first = mixed_out(0)
        gh = [first, mixed_out(1)]

    for k in range(2):
        gm[k].drained()
        stats_sent(k)
    docs_sent()
    half = final.at[:, lanes(h * ds_, ds_)]
    send(state.at[1 - ko], half, f_sem.at[1], f_sem.at[2], zpeer)
    final[:, lanes(h * ds_, ds_)] = state[ko]
    for layer in range(LAYERS):
        for k in range(2):
            tail_sent(layer, k)
    for q in range(parts):
        part_sent(q)
    send_wait(half, f_sem.at[1])
    recv_wait(final.at[:, lanes((1 - h) * ds_, ds_)], f_sem.at[2])
    done = pltpu.make_async_copy(final, out, f_sem.at[0])
    done.start()
    done.wait()


def per_device(
    sizes, hidden, doc_ids, norm_gain, w_value, w_gate, conv_taps, conv_bias, chan_gain, chan_bias, w_out
):
    SP, TP = sizes
    Z, Y = grid_of(SP)
    X = TP // 2
    T = hidden.shape[0]
    D = hidden.shape[1] * TP
    C = w_value.shape[2] * TP
    LAYERS, WIDTH = conv_taps.shape[0], conv_taps.shape[1]
    S = 4 * X
    cs, ds_ = C // S, D // S
    rp, ro = D // SP, C // SP
    bf, f32 = jnp.bfloat16, jnp.float32

    docs = jnp.broadcast_to(doc_ids[:, None], (T, 128))

    dims = (Z, Y, X, T, D, C, LAYERS, WIDTH)
    parts = 2 * LAYERS
    nx, ny = X - 1, Y - 1
    dma = pltpu.SemaphoreType.DMA
    vm = pl.BlockSpec(memory_space=pltpu.VMEM)
    hbm = pl.BlockSpec(memory_space=pl.ANY)
    return pl.pallas_call(
        functools.partial(kernel, dims),
        out_shape=jax.ShapeDtypeStruct((T, 2 * ds_), bf),
        in_specs=[hbm, vm, vm, hbm, hbm, vm, vm, vm, vm, hbm],
        out_specs=hbm,
        scratch_shapes=[
            pltpu.VMEM((LAYERS, SP, rp, 2 * cs), bf),
            pltpu.VMEM((LAYERS, SP, ro, ds_), bf),
            pltpu.VMEM((LAYERS, rp, 4 * cs), bf),
            pltpu.VMEM((LAYERS, ro, 2 * ds_), bf),
            pltpu.VMEM((2, T, D), bf),
            pltpu.VMEM((T, D), bf),
            pltpu.VMEM((2, T, C), bf),
            pltpu.VMEM((T, 2 * cs), f32),
            pltpu.VMEM((T, ds_), f32),
            pltpu.VMEM((2, T + HALO, cs), f32),
            pltpu.VMEM((2, T, cs), f32),
            pltpu.VMEM((2, T, ds_), bf),
            pltpu.VMEM((T, 2 * ds_), bf),
            pltpu.VMEM((LAYERS, 2, HALO, cs), bf),
            pltpu.VMEM((LAYERS, 2, HALO, cs), bf),
            pltpu.VMEM((2, T, 128), f32),
            pltpu.VMEM((2, 8, T), f32),
            pltpu.VMEM((2, 2 * X, 8, T), f32),
            pltpu.VMEM((2, 2, 8, T), f32),
            pltpu.VMEM((LAYERS, HALO, cs), bf),
            pltpu.VMEM((2, T, 128), f32),
            pltpu.VMEM((2, T, 128), jnp.int32),
            pltpu.VMEM((HALO, 128), jnp.int32),
            dma((parts,)),
            dma((parts,)),
            dma((parts,)),
            dma((parts, 3)),
            dma((parts, Z, ny)),
            dma((parts, 2, 3)),
            dma((parts, Z, ny)),
            dma((2, 3 + 4 * nx)),
            dma((2, 4 + 4 * nx)),
            dma((2, 3 + 4 * nx)),
            dma((2, 4 + 4 * nx)),
            dma((2, 2 * X)),
            dma((2, 2 * X)),
            dma((2,)),
            dma((2, 2)),
            dma((LAYERS,)),
            dma((LAYERS,)),
            dma((LAYERS, 2)),
            dma((LAYERS, 2)),
            dma((3,)),
            dma((5,)),
        ],
        compiler_params=pltpu.CompilerParams(has_side_effects=True, vmem_limit_bytes=60 << 20),
        name="stack",
    )(hidden, docs, norm_gain, w_value, w_gate, conv_taps, conv_bias, chan_gain, chan_bias, w_out)


def solution(mesh):
    placed = (
        P("sp", "tp"),
        P("sp"),
        P(),
        P(None, "sp", "tp"),
        P(None, "sp", "tp"),
        P(None, None, "tp"),
        P(None, "tp"),
        P(None, "tp"),
        P(None, "tp"),
        P(None, "sp", "tp"),
    )
    sizes = (mesh.shape["sp"], mesh.shape["tp"])
    return jax.shard_map(
        functools.partial(per_device, sizes),
        mesh=mesh,
        in_specs=placed,
        out_specs=P("sp", "tp"),
        check_vma=False,
    )
```

```python
import functools
import math

import jax
import jax.numpy as jnp
from jax import lax
from jax.experimental import pallas as pl
from jax.experimental.pallas import tpu as pltpu
from jax.sharding import PartitionSpec as P

MESH = pl.DeviceIdType.MESH
HALO = 32
ROWS = 64


def grid_of(size):
    inner = max(d for d in range(1, math.isqrt(size) + 1) if size % d == 0)
    return size // inner, inner


def kernel(
    dims,
    hid,
    docs,
    ngain,
    wv,
    wg,
    taps,
    cbias,
    cgain,
    chbias,
    wo,
    out,
    wp_buf,
    wo_buf,
    stage_p,
    stage_o,
    xg,
    xn,
    mg,
    prod,
    branch,
    glu,
    conv,
    state,
    tail,
    halo,
    stat,
    stat_out,
    stat_in,
    stat_row,
    tail_relay,
    cols,
    pos,
    doc_halo,
    loc_sem,
    g_recv,
    g_send,
    z_recv,
    y_recv,
    z_send,
    y_send,
    h_recv,
    h_send,
    m_recv,
    m_send,
    s_recv,
    s_send,
    r_recv,
    r_send,
    k_recv,
    k_send,
    t_recv,
    t_send,
    f_sem,
    d_sem,
):
    Z, Y, X, T, D, C, LAYERS, WIDTH = dims
    S = 4 * X
    cs, ds_ = C // S, D // S
    parts = 2 * LAYERS
    nx, ny = X - 1, Y - 1

    spi, tpi = lax.axis_index("sp"), lax.axis_index("tp")
    z, y, x, c = spi // Y, spi % Y, tpi // 2, tpi % 2
    zn = z + 1 - 2 * (z % 2)
    zh, ko = z // 2, z % 2
    inner = ((z + 1) // 2) % 2
    h = 1 - inner
    zin = inner * z + h * zn
    zout = h * z + inner * zn
    me = (x * 2 + c) * 2 + h

    def dev(zz, yy, xx, cc):
        return (zz * Y + yy, xx * 2 + cc)

    partner = dev(z, y, x, 1 - c)
    zpeer = dev(zn, y, x, c)

    def send(src, dst, ssem, rsem, device):
        pltpu.make_async_remote_copy(
            src_ref=src, dst_ref=dst, send_sem=ssem, recv_sem=rsem,
            device_id=device, device_id_type=MESH,
        ).start()

    def recv_wait(ref, sem):
        pltpu.make_async_remote_copy(
            src_ref=ref, dst_ref=ref, send_sem=sem, recv_sem=sem,
            device_id=partner, device_id_type=MESH,
        ).wait_recv()

    def send_wait(ref, sem):
        pltpu.make_async_remote_copy(
            src_ref=ref, dst_ref=ref, send_sem=sem, recv_sem=sem,
            device_id=partner, device_id_type=MESH,
        ).wait_send()

    def lanes(start, size):
        return pl.ds(pl.multiple_of(start, 128), size)

    def block(q, b):
        return (wo_buf if q % 2 else wp_buf).at[q // 2, b]

    def own_pieces(q, half, dst, staged=False):
        l = q // 2
        if q % 2:
            src = stage_o if staged else wo
            return [(src.at[l, :, lanes(half * ds_, ds_)], dst)]
        low, high = dst.at[:, pl.ds(0, cs)], dst.at[:, pl.ds(cs, cs)]
        if staged:
            return [
                (stage_p.at[l, :, lanes(half * cs, cs)], low),
                (stage_p.at[l, :, lanes((half + 2) * cs, cs)], high),
            ]
        return [
            (wv.at[l, :, lanes(half * cs, cs)], low),
            (wg.at[l, :, lanes(half * cs, cs)], high),
        ]

    def own_send(q, half, dst, ssem, rsem, device, staged=False):
        for src, part in own_pieces(q, half, dst, staged):
            send(src, part, ssem, rsem, device)

    def hand_over(q):
        l = q // 2
        if q % 2:
            moves = [(wo.at[l], stage_o.at[l])]
        else:
            moves = [
                (wv.at[l], stage_p.at[l, :, pl.ds(0, 2 * cs)]),
                (wg.at[l], stage_p.at[l, :, pl.ds(2 * cs, 2 * cs)]),
            ]
        for src, dst in moves:
            send(src, dst, g_send.at[q], g_recv.at[q], partner)

    def staged_ref(q):
        return (stage_o if q % 2 else stage_p).at[q // 2]

    def z_sends(q, which=(0, 1, 2)):
        mine = block(q, z * Y + y)
        moves = [
            (1 - h, z_recv.at[q, 0], zn),
            (h, z_recv.at[q, 1 + h], Z - 1 - z),
            (1 - h, z_recv.at[q, 1 + h], Z - 1 - zn),
        ]
        for i in which:
            half, rsem, zz = moves[i]
            for cc in (1, 0):
                if i == which[0] and cc == 0 and 1 in which:
                    recv_wait(staged_ref(q), g_recv.at[q])
                own_send(q, half, mine, z_send.at[q, cc, i], rsem, dev(zz, y, x, cc), cc == 0)

    def z_early(*qs):
        @pl.when((c == 1) & (inner == 1))
        def _():
            for q in qs:
                z_sends(q, (1,))

    def z_late(*qs):
        @pl.when((c == 1) & (inner == 1))
        def _():
            for q in qs:
                z_sends(q, (0, 2))

    def z_start(*qs, kind=None):
        @pl.when((c == 1) if kind is None else (c == 1) & (inner == kind))
        def _():
            for q in qs:
                z_sends(q)

    def y_spread(q, zb):
        b = zb * Y + y
        for j in range(1, Y):
            send(block(q, b), block(q, b), y_send.at[q, zb, j - 1], y_recv.at[q, zb, j - 1],
                 dev(z, (y + j) % Y, x, c))

    def start_part(q):
        mine = block(q, z * Y + y)
        for j in range(1, Y):
            own_send(q, h, mine, y_send.at[q, z, j - 1], y_recv.at[q, z, j - 1],
                     dev(z, (y + j) % Y, x, c))
        for src, part in own_pieces(q, h, mine):
            pltpu.make_async_copy(src, part, loc_sem.at[q]).start()

    def event1(q):
        recv_wait(block(q, zn * Y + y), z_recv.at[q, 0])
        y_spread(q, zn)

    def event2(q):
        zb = Z - 1 - zin
        recv_wait(block(q, zb * Y + y), z_recv.at[q, 1])
        y_spread(q, zb)

    def event3(q):
        zb = Z - 1 - zout
        recv_wait(block(q, zb * Y + y), z_recv.at[q, 2])
        y_spread(q, zb)

    def part_ready(q):
        mine = block(q, z * Y + y)
        pltpu.make_async_copy(mine, mine, loc_sem.at[q]).wait()
        for zb in range(Z):
            for j in range(1, Y):
                recv_wait(block(q, zb * Y + (y - j + Y) % Y), y_recv.at[q, zb, j - 1])

    def part_sent(q):
        ref = block(q, 0)
        for zb in range(Z):
            for j in range(1, Y):
                send_wait(ref, y_send.at[q, zb, j - 1])

        @pl.when(c == 1)
        def _():
            for cc in range(2):
                for i in range(3):
                    send_wait(ref, z_send.at[q, cc, i])

        @pl.when(c == 0)
        def _():
            send_wait(staged_ref(q), g_send.at[q])

    class Gather:
        def __init__(self, region, recv, sent, source=None, near=False):
            self.region, self.recv, self.sent, self.near = region, recv, sent, near
            self.own = region(x, c, z)
            self.source = self.own if source is None else source

        def xs(self, j):
            return (x - j + X) % X

        def forward(self, ref, i, device):
            send(ref, ref, self.sent.at[i], self.recv.at[i], device)

        def first(self):
            def go(i, device):
                send(self.source, self.own, self.sent.at[i], self.recv.at[i], device)

            for j in range(1, X):
                go(2 + j, dev(z, y, (x + j) % X, c))
            go(0, partner)

            @pl.when(c == 0)
            def _():
                go(1, zpeer)

        def across(self):
            @pl.when(c == 0)
            def _():
                ref = self.region(x, 1, z)
                recv_wait(ref, self.recv.at[0])
                send(ref, ref, self.sent.at[3 + 4 * nx], self.recv.at[1], dev(zn, y, x, 1))

        def second(self):
            ref = self.region(x, c, zn)
            recv_wait(ref, self.recv.at[1])
            for j in range(1, X):
                if not self.near:
                    self.forward(ref, 2 + nx + j, dev(z, y, (x + j) % X, c))
            self.forward(ref, 2, partner)

        def third(self):
            for j in range(1, X):
                ref = self.region(self.xs(j), c, z)
                recv_wait(ref, self.recv.at[2 + j])
                self.forward(ref, 2 + 2 * nx + j, partner)

        def beyond(self):
            @pl.when(c == 0)
            def _():
                for j in range(1, X):
                    recv_wait(self.region(self.xs(j), 1, z), self.recv.at[2 + 2 * nx + j])
                    for cc in range(2):
                        ref = self.region(self.xs(j), cc, z)
                        send(ref, ref, self.sent.at[2 + 4 * nx + 2 * j + cc], self.recv.at[2 + nx + j],
                             dev(zn, y, x, cc))

        def fourth(self):
            for j in range(1, X):
                ref = self.region(self.xs(j), c, zn)
                recv_wait(ref, self.recv.at[2 + nx + j])
                self.forward(ref, 2 + 3 * nx + j, partner)

        def last(self):
            @pl.when(c == 1)
            def _():
                recv_wait(self.region(x, 0, z), self.recv.at[0])

            recv_wait(self.region(x, 1 - c, zn), self.recv.at[2])
            for j in range(1, X):
                if self.near:
                    @pl.when(c == 1)
                    def _():
                        recv_wait(self.region(self.xs(j), 0, z), self.recv.at[2 + 2 * nx + j])
                else:
                    recv_wait(self.region(self.xs(j), 1 - c, z), self.recv.at[2 + 2 * nx + j])
                recv_wait(self.region(self.xs(j), 1 - c, zn), self.recv.at[2 + 3 * nx + j])

        def drained(self):
            for i in [0] + list(range(2, 3 + 4 * nx)):
                if not (self.near and 3 + nx <= i < 3 + 2 * nx):
                    send_wait(self.own, self.sent.at[i])

            @pl.when(c == 0)
            def _():
                send_wait(self.own, self.sent.at[1])
                send_wait(self.own, self.sent.at[3 + 4 * nx])
                if self.near:
                    for i in range(2 * nx):
                        send_wait(self.own, self.sent.at[4 + 4 * nx + i])

    def slot(xx, cc, zz):
        return (xx * 2 + cc) * 2 + 1 - ((zz + 1) // 2) % 2

    def hidden_gather(layer, k):
        if layer == 0:
            return Gather(
                lambda xx, cc, zz: xg.at[zz % 2, :, lanes((xx * 2 + cc) * 2 * ds_, 2 * ds_)],
                h_recv.at[0], h_send.at[0], hid,
            )
        return Gather(
            lambda xx, cc, zz: xg.at[k, :, lanes(slot(xx, cc, zz) * ds_, ds_)],
            h_recv.at[k], h_send.at[k], state.at[k], k == 1 and layer == LAYERS - 1,
        )

    def mixed_gather(layer, k):
        return Gather(
            lambda xx, cc, zz: mg.at[k, :, lanes(slot(xx, cc, zz) * cs, cs)],
            m_recv.at[k], m_send.at[k], near=k == 1 and layer == LAYERS - 1,
        )

    def normalise(layer, k):
        @pl.loop(0, T // 16, unroll=2)
        def _(i):
            rows = pl.ds(pl.multiple_of(i * 16, 16), 16)
            v = xg[k, rows, :].astype(jnp.float32)
            scale = lax.rsqrt(jnp.mean(v * v, axis=-1, keepdims=True) + 1e-6)
            cols[0, rows, :] = jnp.broadcast_to(scale, (16, 128))

        @pl.loop(0, T // 16)
        def _(i):
            rows = pl.ds(pl.multiple_of(i * 16, 16), 16)
            scale = cols[0, rows, :]
            for t in range(D // 128):
                at = slice(t * 128, (t + 1) * 128)
                v = xg[k, rows, at].astype(jnp.float32) * scale * ngain[layer : layer + 1, at]
                xn[rows, at] = v.astype(jnp.bfloat16)

    def matmul(acc, lhs, rhs, depth, count):
        acc[...] = jnp.zeros_like(acc)

        @pl.loop(0, count)
        def _(b):
            acc[...] += jnp.dot(
                lhs[:, lanes(b * depth, depth)], rhs[b], preferred_element_type=jnp.float32
            )

    def project(layer, k):
        matmul(prod, xn, wp_buf.at[layer], D // (Z * Y), Z * Y)

        @pl.loop(0, T // HALO)
        def _(i):
            rows = pl.ds(pl.multiple_of(i * HALO, HALO), HALO)
            v, g = prod[rows, 0:cs], prod[rows, cs : 2 * cs]
            r = (v * jax.nn.sigmoid(g)).astype(jnp.bfloat16)
            glu[k, pl.ds(pl.multiple_of(i * HALO + HALO, HALO), HALO), :] = r.astype(jnp.float32)

    def project_tail(layer, k):
        rows = slice(T - HALO, T)

        def step(b, acc):
            lhs = xn[rows, lanes(b * (D // (Z * Y)), D // (Z * Y))]
            return acc + jnp.dot(lhs, wp_buf[layer, b], preferred_element_type=jnp.float32)

        both = lax.fori_loop(0, Z * Y, step, jnp.zeros((HALO, 2 * cs), jnp.float32))
        tail[layer, k] = (both[:, 0:cs] * jax.nn.sigmoid(both[:, cs:])).astype(jnp.bfloat16)

    def tail_send(layer, k):
        def go(kk, device):
            send(tail.at[layer, k], halo.at[layer, kk], t_send.at[layer, k], t_recv.at[layer, kk], device)

        @pl.when(y < Y - 1)
        def _():
            go(k, dev(z, y + 1, x, c))

        if k == 0:
            @pl.when(y == Y - 1)
            def _():
                go(1, dev(z, 0, x, c))
        else:
            @pl.when((y == Y - 1) & (zh == 0) & (c == 0))
            def _():
                go(0, dev(Z - 1 - z, 0, x, 0))
                recv_wait(tail_relay.at[layer], k_recv.at[layer])
                send(tail_relay.at[layer], halo.at[layer, 0], k_send.at[layer], t_recv.at[layer, 0],
                     dev(Z - 1 - z, 0, x, 1))

            @pl.when((y == Y - 1) & (zh == 0) & (c == 1))
            def _():
                send(tail.at[layer, k], tail_relay.at[layer], t_send.at[layer, k], k_recv.at[layer], partner)

    def tail_sent(layer, k):
        if k == 0:
            send_wait(tail.at[layer, k], t_send.at[layer, k])
        else:
            @pl.when((y < Y - 1) | (zh == 0))
            def _():
                send_wait(tail.at[layer, k], t_send.at[layer, k])

            @pl.when((y == Y - 1) & (zh == 0) & (c == 0))
            def _():
                send_wait(tail_relay.at[layer], k_send.at[layer])

    def tail_recv(layer, k):
        def arrive():
            recv_wait(halo.at[layer, k], t_recv.at[layer, k])
            glu[k, 0:HALO, :] = halo[layer, k].astype(jnp.float32)

        if k == 1:
            arrive()
        else:
            @pl.when((y > 0) | (zh > 0))
            def _():
                arrive()

            @pl.when((y == 0) & (zh == 0))
            def _():
                glu[k, 0:HALO, :] = jnp.zeros((HALO, cs), jnp.float32)

    def convolve_tile(layer, k, base):
        first_lane = lax.broadcasted_iota(jnp.int32, (ROWS, 128), 1) == 0
        near = pos[k, pl.ds(base, ROWS), :]
        total = jnp.zeros((ROWS, 128), jnp.float32)
        square = jnp.zeros((ROWS, 128), jnp.float32)
        for t in range(cs // 128):
            at = lanes(h * cs + t * 128, 128)
            span = glu[k, pl.ds(base, ROWS + HALO), t * 128 : (t + 1) * 128]
            acc = jnp.broadcast_to(cbias[layer : layer + 1, at], (ROWS, 128))
            for phase in range(8):
                moved = span if phase == 0 else pltpu.roll(span, ROWS + HALO - phase, 0)
                for off in range(phase, HALO + 1, 8):
                    index = off - (HALO - (WIDTH - 1))
                    if 0 <= index < WIDTH:
                        start = off - phase
                        term = moved[start : start + ROWS] * taps[layer, index : index + 1, at]
                        back = WIDTH - 1 - index
                        acc = acc + (jnp.where(near >= back, term, 0.0) if back else term)
            conv[k, pl.ds(base, ROWS), t * 128 : (t + 1) * 128] = acc
            total = total + acc
            square = square + acc * acc
        s1 = jnp.sum(total, axis=1, keepdims=True)
        s2 = jnp.sum(square, axis=1, keepdims=True)
        stat[k, pl.ds(base, ROWS), :] = jnp.where(first_lane, s1, s2)

    def convolve(layer, k):
        @pl.loop(1, T // ROWS)
        def _(i):
            convolve_tile(layer, k, pl.multiple_of(i * ROWS, ROWS))

    def convolve_first(layer, k):
        convolve_tile(layer, k, 0)
        for t in range(T // 128):
            stat_out[k, :, t * 128 : (t + 1) * 128] = stat[k, t * 128 : (t + 1) * 128, :].T[0:8, :]

    def others():
        for xj in range(X):
            for cj in range(2):
                if xj or cj:
                    device = dev(z, y, (x + xj) % X, (c + cj) % 2)
                    yield xj * 2 + cj, device, (x - xj + X) % X * 2 + (c + cj) % 2

    def stats_send(k):
        for i, device, _ in others():
            send(stat_out.at[k], stat_in.at[k, x * 2 + c], s_send.at[k, i], s_recv.at[k, i], device)

    def row_sum(k):
        for i, _, theirs in others():
            recv_wait(stat_in.at[k, theirs], s_recv.at[k, i])
        stat_in[k, x * 2 + c] = stat_out[k]
        total = stat_in[k, 0]
        for i in range(1, 2 * X):
            total = total + stat_in[k, i]
        stat_row[k, h] = total

        @pl.when(c == 0)
        def _():
            for cc in range(2):
                send(stat_row.at[k, h], stat_row.at[k, h], r_send.at[k, cc], r_recv.at[k], dev(zn, y, x, cc))

    def mix(layer, k):
        recv_wait(stat_row.at[k, 1 - h], r_recv.at[k])
        total = stat_row[k, 0] + stat_row[k, 1]
        for t in range(T // 128):
            tile = total[:, t * 128 : (t + 1) * 128]
            turned = jnp.concatenate([tile] * 16, axis=0).T
            mu = turned[:, 0:1] * (1.0 / C)
            var = turned[:, 1:2] * (1.0 / C) - mu * mu
            rows = slice(t * 128, (t + 1) * 128)
            cols[0, rows, :] = jnp.broadcast_to(mu, (128, 128))
            cols[1, rows, :] = jnp.broadcast_to(lax.rsqrt(var + 1e-5), (128, 128))

        @pl.loop(0, T // ROWS)
        def _(i):
            rows = pl.ds(pl.multiple_of(i * ROWS, ROWS), ROWS)
            mu, scale = cols[0, rows, :], cols[1, rows, :]
            for t in range(cs // 128):
                at = lanes(h * cs + t * 128, 128)
                v = (conv[k, rows, t * 128 : (t + 1) * 128] - mu) * scale
                v = v * cgain[layer : layer + 1, at] + chbias[layer : layer + 1, at]
                mg[k, rows, lanes(me * cs + t * 128, 128)] = jax.nn.silu(v).astype(jnp.bfloat16)

    def stats_sent(k):
        for i, _, _ in others():
            send_wait(stat_out.at[k], s_send.at[k, i])

        @pl.when(c == 0)
        def _():
            for cc in range(2):
                send_wait(stat_row.at[k, h], r_send.at[k, cc])

    def contract(layer, k):
        matmul(branch, mg.at[k], wo_buf.at[layer], C // (Z * Y), Z * Y)
        state[k] = (state[k].astype(jnp.float32) + branch[...]).astype(jnp.bfloat16)

    def docs_start():
        tail_docs = docs.at[pl.ds(T - HALO, HALO)]

        @pl.when(y < Y - 1)
        def _():
            send(tail_docs, doc_halo, d_sem.at[0], d_sem.at[1], dev(z, y + 1, x, c))

        @pl.when((y == Y - 1) & (z < Z - 1))
        def _():
            send(tail_docs, doc_halo, d_sem.at[0], d_sem.at[1], dev(z + 1, 0, x, c))

    def docs_done():
        @pl.when((y > 0) | (z > 0))
        def _():
            recv_wait(doc_halo, d_sem.at[1])

        @pl.when((y == 0) & (z == 0))
        def _():
            doc_halo[...] = jnp.full((HALO, 128), -1, jnp.int32)

        def count(base, span):
            here = span[HALO:]
            total = jnp.zeros((ROWS, 128), jnp.int32)
            for phase in range(8):
                moved = span if phase == 0 else pltpu.roll(span, ROWS + HALO - phase, 0)
                for off in range(phase, HALO, 8):
                    if off >= HALO - (WIDTH - 1):
                        start = off - phase
                        same = moved[start : start + ROWS] == here
                        total = total + jnp.where(same, 1, 0)
            pos[ko, pl.ds(base, ROWS), :] = total

        count(0, jnp.concatenate([doc_halo[...], docs[0:ROWS, :]], axis=0))

        @pl.loop(1, T // ROWS)
        def _(i):
            base = pl.multiple_of(i * ROWS, ROWS)
            count(base, docs[pl.ds(pl.multiple_of(base - HALO, HALO), ROWS + HALO), :])

        @pl.when(c == 0)
        def _():
            send(pos.at[ko], pos.at[ko], d_sem.at[2], d_sem.at[3], dev(zn, y, x, 0))
            send(pos.at[ko], pos.at[ko], d_sem.at[4], d_sem.at[3], dev(zn, y, x, 1))

    def docs_sent():
        @pl.when((y < Y - 1) | (z < Z - 1))
        def _():
            send_wait(doc_halo, d_sem.at[0])

        @pl.when(c == 0)
        def _():
            send_wait(pos.at[ko], d_sem.at[2])
            send_wait(pos.at[ko], d_sem.at[4])

    own0 = xg.at[ko, :, lanes((x * 2 + c) * 2 * ds_, 2 * ds_)]
    local = pltpu.make_async_copy(hid, own0, f_sem.at[0])
    local.start()
    docs_start()

    @pl.when(c == 0)
    def _():
        for q in range(parts):
            hand_over(q)

    start_part(0)

    z_start(0)

    gh = [hidden_gather(0, 0)]
    gh[0].first()
    gh[0].across()
    docs_done()
    event1(0)
    event2(0)
    gh[0].third()
    gh[0].second()
    local.wait()
    z_start(1, 2, kind=0)
    event3(0)
    z_start(1, 2, kind=1)
    start_part(1)

    gm = None
    for layer in range(LAYERS):
        p_now, o_now, p_next = 2 * layer, 2 * layer + 1, 2 * layer + 2
        more = layer + 1 < LAYERS

        def mixed_out(k):
            gm[k].fourth()
            gm[k].last()
            if k == 0:
                part_ready(o_now)
            contract(layer, k)
            if more:
                xg[k, :, lanes(me * ds_, ds_)] = state[k]
                gather = hidden_gather(layer + 1, k)
                gather.first()
                gather.across()
                return gather

        if layer:
            bulk = [o_now, p_next] if more else [o_now]
            z_early(*bulk)
            gh[0].second()
            gh[0].third()
            if layer == 1:
                event2(p_now)
            else:

                @pl.when(inner == 0)
                def _():
                    event2(p_now)

            event3(p_now)
            start_part(o_now)
            gh[1].third()
            if not more:
                gh[1].beyond()
            gh[1].second()
            z_start(*bulk, kind=0)
        for k in range(2):
            if k < len(gh):
                gh[k].fourth()
                gh[k].last()
            if layer and k == 0:
                z_late(*bulk)
            if layer == 0 and k == 0:
                for kk in range(2):
                    state[kk] = xg[kk, :, lanes(me * ds_, ds_)]
            normalise(layer, k)
            if k == 0:
                part_ready(p_now)
            if k:
                project_tail(layer, k)
                tail_send(layer, k)
            project(layer, k)
            if k == 0:
                tail[layer, k] = glu[k, T : T + HALO, :].astype(jnp.bfloat16)
                tail_send(layer, k)
            if k < len(gh):
                gh[k].drained()
            if k == 0:
                if layer == 0:
                    recv_wait(pos.at[1 - ko], d_sem.at[3])
                else:
                    stats_sent(0)
                    stats_sent(1)
            convolve(layer, k)
            if k == 0 and layer == 0:
                event1(o_now)

                @pl.when(inner == 1)
                def _():
                    event2(o_now)

        for k in range(2):
            tail_recv(layer, k)
            convolve_first(layer, k)
            if layer:
                gm[k].drained()
            stats_send(k)
        if layer:
            event1(o_now)
            event2(o_now)
        else:

            @pl.when(inner == 0)
            def _():
                event2(o_now)

        for k in range(2):
            row_sum(k)
        gm = [mixed_gather(layer, k) for k in range(2)]
        for k in range(2):
            mix(layer, k)
            gm[k].first()
            gm[k].across()
        event3(o_now)
        if more:
            start_part(p_next)
            if layer == 0:
                event1(p_next)
            else:

                @pl.when(inner == 1)
                def _():
                    event1(p_next)

        gm[0].third()
        gm[0].second()
        gm[1].third()
        if not more:
            gm[1].beyond()
        gm[1].second()
        first = mixed_out(0)
        if more and layer:

            @pl.when(inner == 1)
            def _():
                event2(p_next)

            @pl.when(inner == 0)
            def _():
                event1(p_next)

        gh = [first, mixed_out(1)]

    for k in range(2):
        gm[k].drained()
        stats_sent(k)
    docs_sent()
    half = out.at[:, lanes(h * ds_, ds_)]
    send(state.at[1 - ko], half, f_sem.at[1], f_sem.at[2], zpeer)
    done = pltpu.make_async_copy(state.at[ko], half, f_sem.at[0])
    done.start()
    for layer in range(LAYERS):
        for k in range(2):
            tail_sent(layer, k)
    for q in range(parts):
        part_sent(q)
    send_wait(half, f_sem.at[1])
    done.wait()
    recv_wait(out.at[:, lanes((1 - h) * ds_, ds_)], f_sem.at[2])


def per_device(
    sizes, hidden, doc_ids, norm_gain, w_value, w_gate, conv_taps, conv_bias, chan_gain, chan_bias, w_out
):
    SP, TP = sizes
    Z, Y = grid_of(SP)
    X = TP // 2
    T = hidden.shape[0]
    D = hidden.shape[1] * TP
    C = w_value.shape[2] * TP
    LAYERS, WIDTH = conv_taps.shape[0], conv_taps.shape[1]
    S = 4 * X
    cs, ds_ = C // S, D // S
    rp, ro = D // SP, C // SP
    bf, f32 = jnp.bfloat16, jnp.float32

    docs = jnp.broadcast_to(doc_ids[:, None], (T, 128))

    dims = (Z, Y, X, T, D, C, LAYERS, WIDTH)
    parts = 2 * LAYERS
    nx, ny = X - 1, Y - 1
    dma = pltpu.SemaphoreType.DMA
    vm = pl.BlockSpec(memory_space=pltpu.VMEM)
    hbm = pl.BlockSpec(memory_space=pl.ANY)
    return pl.pallas_call(
        functools.partial(kernel, dims),
        out_shape=jax.ShapeDtypeStruct((T, 2 * ds_), bf),
        in_specs=[hbm, vm, vm, hbm, hbm, vm, vm, vm, vm, hbm],
        out_specs=hbm,
        scratch_shapes=[
            pltpu.VMEM((LAYERS, SP, rp, 2 * cs), bf),
            pltpu.VMEM((LAYERS, SP, ro, ds_), bf),
            pltpu.VMEM((LAYERS, rp, 4 * cs), bf),
            pltpu.VMEM((LAYERS, ro, 2 * ds_), bf),
            pltpu.VMEM((2, T, D), bf),
            pltpu.VMEM((T, D), bf),
            pltpu.VMEM((2, T, C), bf),
            pltpu.VMEM((T, 2 * cs), f32),
            pltpu.VMEM((T, ds_), f32),
            pltpu.VMEM((2, T + HALO, cs), f32),
            pltpu.VMEM((2, T, cs), f32),
            pltpu.VMEM((2, T, ds_), bf),
            pltpu.VMEM((LAYERS, 2, HALO, cs), bf),
            pltpu.VMEM((LAYERS, 2, HALO, cs), bf),
            pltpu.VMEM((2, T, 128), f32),
            pltpu.VMEM((2, 8, T), f32),
            pltpu.VMEM((2, 2 * X, 8, T), f32),
            pltpu.VMEM((2, 2, 8, T), f32),
            pltpu.VMEM((LAYERS, HALO, cs), bf),
            pltpu.VMEM((2, T, 128), f32),
            pltpu.VMEM((2, T, 128), jnp.int32),
            pltpu.VMEM((HALO, 128), jnp.int32),
            dma((parts,)),
            dma((parts,)),
            dma((parts,)),
            dma((parts, 3)),
            dma((parts, Z, ny)),
            dma((parts, 2, 3)),
            dma((parts, Z, ny)),
            dma((2, 3 + 4 * nx)),
            dma((2, 4 + 6 * nx)),
            dma((2, 3 + 4 * nx)),
            dma((2, 4 + 6 * nx)),
            dma((2, 2 * X)),
            dma((2, 2 * X)),
            dma((2,)),
            dma((2, 2)),
            dma((LAYERS,)),
            dma((LAYERS,)),
            dma((LAYERS, 2)),
            dma((LAYERS, 2)),
            dma((3,)),
            dma((5,)),
        ],
        compiler_params=pltpu.CompilerParams(has_side_effects=True, vmem_limit_bytes=60 << 20),
        name="stack",
    )(hidden, docs, norm_gain, w_value, w_gate, conv_taps, conv_bias, chan_gain, chan_bias, w_out)


def solution(mesh):
    placed = (
        P("sp", "tp"),
        P("sp"),
        P(),
        P(None, "sp", "tp"),
        P(None, "sp", "tp"),
        P(None, None, "tp"),
        P(None, "tp"),
        P(None, "tp"),
        P(None, "tp"),
        P(None, "sp", "tp"),
    )
    sizes = (mesh.shape["sp"], mesh.shape["tp"])
    return jax.shard_map(
        functools.partial(per_device, sizes),
        mesh=mesh,
        in_specs=placed,
        out_specs=P("sp", "tp"),
        check_vma=False,
    )
```

```python
import functools
import math

import jax
import jax.numpy as jnp
from jax import lax
from jax.experimental import pallas as pl
from jax.experimental.pallas import tpu as pltpu
from jax.sharding import PartitionSpec as P

MESH = pl.DeviceIdType.MESH
HALO = 32
ROWS = 64


def grid_of(size):
    inner = max(d for d in range(1, math.isqrt(size) + 1) if size % d == 0)
    return size // inner, inner


def kernel(
    dims,
    hid,
    docs,
    ngain,
    wv,
    wg,
    taps,
    cbias,
    cgain,
    chbias,
    wo,
    out,
    wp_buf,
    wo_buf,
    stage_p,
    stage_o,
    xg,
    xn,
    mg,
    prod,
    branch,
    glu,
    conv,
    state,
    tail,
    halo,
    stat,
    stat_out,
    stat_in,
    stat_row,
    tail_relay,
    cols,
    pos,
    doc_halo,
    loc_sem,
    g_recv,
    g_send,
    z_recv,
    y_recv,
    z_send,
    y_send,
    h_recv,
    h_send,
    m_recv,
    m_send,
    s_recv,
    s_send,
    r_recv,
    r_send,
    k_recv,
    k_send,
    t_recv,
    t_send,
    f_sem,
    d_sem,
):
    Z, Y, X, T, D, C, LAYERS, WIDTH = dims
    S = 4 * X
    cs, ds_ = C // S, D // S
    parts = 2 * LAYERS
    nx, ny = X - 1, Y - 1

    spi, tpi = lax.axis_index("sp"), lax.axis_index("tp")
    z, y, x, c = spi // Y, spi % Y, tpi // 2, tpi % 2
    zn = z + 1 - 2 * (z % 2)
    zh, ko = z // 2, z % 2
    inner = ((z + 1) // 2) % 2
    h = 1 - inner
    zin = inner * z + h * zn
    zout = h * z + inner * zn
    me = (x * 2 + c) * 2 + h

    def dev(zz, yy, xx, cc):
        return (zz * Y + yy, xx * 2 + cc)

    partner = dev(z, y, x, 1 - c)
    zpeer = dev(zn, y, x, c)

    def send(src, dst, ssem, rsem, device):
        pltpu.make_async_remote_copy(
            src_ref=src, dst_ref=dst, send_sem=ssem, recv_sem=rsem,
            device_id=device, device_id_type=MESH,
        ).start()

    def recv_wait(ref, sem):
        pltpu.make_async_remote_copy(
            src_ref=ref, dst_ref=ref, send_sem=sem, recv_sem=sem,
            device_id=partner, device_id_type=MESH,
        ).wait_recv()

    def send_wait(ref, sem):
        pltpu.make_async_remote_copy(
            src_ref=ref, dst_ref=ref, send_sem=sem, recv_sem=sem,
            device_id=partner, device_id_type=MESH,
        ).wait_send()

    def lanes(start, size):
        return pl.ds(pl.multiple_of(start, 128), size)

    def block(q, b):
        return (wo_buf if q % 2 else wp_buf).at[q // 2, b]

    def own_pieces(q, half, dst, staged=False):
        l = q // 2
        if q % 2:
            src = stage_o if staged else wo
            return [(src.at[l, :, lanes(half * ds_, ds_)], dst)]
        low, high = dst.at[:, pl.ds(0, cs)], dst.at[:, pl.ds(cs, cs)]
        if staged:
            return [
                (stage_p.at[l, :, lanes(half * cs, cs)], low),
                (stage_p.at[l, :, lanes((half + 2) * cs, cs)], high),
            ]
        return [
            (wv.at[l, :, lanes(half * cs, cs)], low),
            (wg.at[l, :, lanes(half * cs, cs)], high),
        ]

    def own_send(q, half, dst, ssem, rsem, device, staged=False):
        for src, part in own_pieces(q, half, dst, staged):
            send(src, part, ssem, rsem, device)

    def hand_over(q):
        l = q // 2
        if q % 2:
            moves = [(wo.at[l], stage_o.at[l])]
        else:
            moves = [
                (wv.at[l], stage_p.at[l, :, pl.ds(0, 2 * cs)]),
                (wg.at[l], stage_p.at[l, :, pl.ds(2 * cs, 2 * cs)]),
            ]
        for src, dst in moves:
            send(src, dst, g_send.at[q], g_recv.at[q], partner)

    def staged_ref(q):
        return (stage_o if q % 2 else stage_p).at[q // 2]

    def z_sends(q, which=(0, 1, 2)):
        mine = block(q, z * Y + y)
        moves = [
            (1 - h, z_recv.at[q, 0], zn),
            (h, z_recv.at[q, 1 + h], Z - 1 - z),
            (1 - h, z_recv.at[q, 1 + h], Z - 1 - zn),
        ]
        for i in which:
            half, rsem, zz = moves[i]
            for cc in (1, 0):
                if i == which[0] and cc == 0 and 1 in which:
                    recv_wait(staged_ref(q), g_recv.at[q])
                own_send(q, half, mine, z_send.at[q, cc, i], rsem, dev(zz, y, x, cc), cc == 0)

    def z_early(*qs):
        @pl.when((c == 1) & (inner == 1))
        def _():
            for q in qs:
                z_sends(q, (1,))

    def z_late(*qs):
        @pl.when((c == 1) & (inner == 1))
        def _():
            for q in qs:
                z_sends(q, (0, 2))

    def z_start(*qs, kind=None):
        @pl.when((c == 1) if kind is None else (c == 1) & (inner == kind))
        def _():
            for q in qs:
                z_sends(q)

    def y_spread(q, zb):
        b = zb * Y + y
        for j in range(1, Y):
            send(block(q, b), block(q, b), y_send.at[q, zb, j - 1], y_recv.at[q, zb, j - 1],
                 dev(z, (y + j) % Y, x, c))

    def start_part(q):
        mine = block(q, z * Y + y)
        for j in range(1, Y):
            own_send(q, h, mine, y_send.at[q, z, j - 1], y_recv.at[q, z, j - 1],
                     dev(z, (y + j) % Y, x, c))
        for src, part in own_pieces(q, h, mine):
            pltpu.make_async_copy(src, part, loc_sem.at[q]).start()

    def event1(q):
        recv_wait(block(q, zn * Y + y), z_recv.at[q, 0])
        y_spread(q, zn)

    def event2(q):
        zb = Z - 1 - zin
        recv_wait(block(q, zb * Y + y), z_recv.at[q, 1])
        y_spread(q, zb)

    def event3(q):
        zb = Z - 1 - zout
        recv_wait(block(q, zb * Y + y), z_recv.at[q, 2])
        y_spread(q, zb)

    def part_ready(q):
        mine = block(q, z * Y + y)
        pltpu.make_async_copy(mine, mine, loc_sem.at[q]).wait()
        for zb in range(Z):
            for j in range(1, Y):
                recv_wait(block(q, zb * Y + (y - j + Y) % Y), y_recv.at[q, zb, j - 1])

    def part_sent(q):
        ref = block(q, 0)
        for zb in range(Z):
            for j in range(1, Y):
                send_wait(ref, y_send.at[q, zb, j - 1])

        @pl.when(c == 1)
        def _():
            for cc in range(2):
                for i in range(3):
                    send_wait(ref, z_send.at[q, cc, i])

        @pl.when(c == 0)
        def _():
            send_wait(staged_ref(q), g_send.at[q])

    class Gather:
        def __init__(self, region, recv, sent, source=None, near=False):
            self.region, self.recv, self.sent, self.near = region, recv, sent, near
            self.own = region(x, c, z)
            self.source = self.own if source is None else source

        def xs(self, j):
            return (x - j + X) % X

        def forward(self, ref, i, device):
            send(ref, ref, self.sent.at[i], self.recv.at[i], device)

        def first(self):
            def go(i, device):
                send(self.source, self.own, self.sent.at[i], self.recv.at[i], device)

            for j in range(1, X):
                go(2 + j, dev(z, y, (x + j) % X, c))
            go(0, partner)

            @pl.when(c == 0)
            def _():
                go(1, zpeer)

        def across(self):
            @pl.when(c == 0)
            def _():
                ref = self.region(x, 1, z)
                recv_wait(ref, self.recv.at[0])
                send(ref, ref, self.sent.at[3 + 4 * nx], self.recv.at[1], dev(zn, y, x, 1))

        def second(self):
            ref = self.region(x, c, zn)
            recv_wait(ref, self.recv.at[1])
            for j in range(1, X):
                if not self.near:
                    self.forward(ref, 2 + nx + j, dev(z, y, (x + j) % X, c))
            self.forward(ref, 2, partner)

        def third(self):
            for j in range(1, X):
                ref = self.region(self.xs(j), c, z)
                recv_wait(ref, self.recv.at[2 + j])
                self.forward(ref, 2 + 2 * nx + j, partner)

        def beyond(self):
            @pl.when(c == 0)
            def _():
                for j in range(1, X):
                    recv_wait(self.region(self.xs(j), 1, z), self.recv.at[2 + 2 * nx + j])
                    for cc in range(2):
                        ref = self.region(self.xs(j), cc, z)
                        send(ref, ref, self.sent.at[2 + 4 * nx + 2 * j + cc], self.recv.at[2 + nx + j],
                             dev(zn, y, x, cc))

        def fourth(self):
            for j in range(1, X):
                ref = self.region(self.xs(j), c, zn)
                recv_wait(ref, self.recv.at[2 + nx + j])
                self.forward(ref, 2 + 3 * nx + j, partner)

        def last(self):
            @pl.when(c == 1)
            def _():
                recv_wait(self.region(x, 0, z), self.recv.at[0])

            recv_wait(self.region(x, 1 - c, zn), self.recv.at[2])
            for j in range(1, X):
                if self.near:
                    @pl.when(c == 1)
                    def _():
                        recv_wait(self.region(self.xs(j), 0, z), self.recv.at[2 + 2 * nx + j])
                else:
                    recv_wait(self.region(self.xs(j), 1 - c, z), self.recv.at[2 + 2 * nx + j])
                recv_wait(self.region(self.xs(j), 1 - c, zn), self.recv.at[2 + 3 * nx + j])

        def drained(self):
            for i in [0] + list(range(2, 3 + 4 * nx)):
                if not (self.near and 3 + nx <= i < 3 + 2 * nx):
                    send_wait(self.own, self.sent.at[i])

            @pl.when(c == 0)
            def _():
                send_wait(self.own, self.sent.at[1])
                send_wait(self.own, self.sent.at[3 + 4 * nx])
                if self.near:
                    for i in range(2 * nx):
                        send_wait(self.own, self.sent.at[4 + 4 * nx + i])

    def slot(xx, cc, zz):
        return (xx * 2 + cc) * 2 + 1 - ((zz + 1) // 2) % 2

    def hidden_gather(layer, k):
        if layer == 0:
            return Gather(
                lambda xx, cc, zz: xg.at[zz % 2, :, lanes((xx * 2 + cc) * 2 * ds_, 2 * ds_)],
                h_recv.at[0], h_send.at[0], hid,
            )
        return Gather(
            lambda xx, cc, zz: xg.at[k, :, lanes(slot(xx, cc, zz) * ds_, ds_)],
            h_recv.at[k], h_send.at[k], state.at[k], k == 1 and layer == LAYERS - 1,
        )

    def mixed_gather(layer, k):
        return Gather(
            lambda xx, cc, zz: mg.at[k, :, lanes(slot(xx, cc, zz) * cs, cs)],
            m_recv.at[k], m_send.at[k], near=k == 1 and layer == LAYERS - 1,
        )

    def normalise(layer, k):
        @pl.loop(0, T // 16, unroll=2)
        def _(i):
            rows = pl.ds(pl.multiple_of(i * 16, 16), 16)
            v = xg[k, rows, :].astype(jnp.float32)
            scale = lax.rsqrt(jnp.mean(v * v, axis=-1, keepdims=True) + 1e-6)
            cols[0, rows, :] = jnp.broadcast_to(scale, (16, 128))

        @pl.loop(0, T // 16)
        def _(i):
            rows = pl.ds(pl.multiple_of(i * 16, 16), 16)
            scale = cols[0, rows, :]
            for t in range(D // 128):
                at = slice(t * 128, (t + 1) * 128)
                v = xg[k, rows, at].astype(jnp.float32) * scale * ngain[layer : layer + 1, at]
                xn[rows, at] = v.astype(jnp.bfloat16)

    def matmul(acc, lhs, rhs, depth, count):
        acc[...] = jnp.zeros_like(acc)

        @pl.loop(0, count)
        def _(b):
            acc[...] += jnp.dot(
                lhs[:, lanes(b * depth, depth)], rhs[b], preferred_element_type=jnp.float32
            )

    def project(layer, k):
        matmul(prod, xn, wp_buf.at[layer], D // (Z * Y), Z * Y)

        @pl.loop(0, T // HALO)
        def _(i):
            rows = pl.ds(pl.multiple_of(i * HALO, HALO), HALO)
            v, g = prod[rows, 0:cs], prod[rows, cs : 2 * cs]
            r = (v * jax.nn.sigmoid(g)).astype(jnp.bfloat16)
            glu[k, pl.ds(pl.multiple_of(i * HALO + HALO, HALO), HALO), :] = r.astype(jnp.float32)

    def tail_send(layer, k):
        def go(kk, device):
            send(tail.at[layer, k], halo.at[layer, kk], t_send.at[layer, k], t_recv.at[layer, kk], device)

        @pl.when(y < Y - 1)
        def _():
            go(k, dev(z, y + 1, x, c))

        if k == 0:
            @pl.when(y == Y - 1)
            def _():
                go(1, dev(z, 0, x, c))
        else:
            @pl.when((y == Y - 1) & (zh == 0) & (c == 0))
            def _():
                go(0, dev(Z - 1 - z, 0, x, 0))
                recv_wait(tail_relay.at[layer], k_recv.at[layer])
                send(tail_relay.at[layer], halo.at[layer, 0], k_send.at[layer], t_recv.at[layer, 0],
                     dev(Z - 1 - z, 0, x, 1))

            @pl.when((y == Y - 1) & (zh == 0) & (c == 1))
            def _():
                send(tail.at[layer, k], tail_relay.at[layer], t_send.at[layer, k], k_recv.at[layer], partner)

    def tail_sent(layer, k):
        if k == 0:
            send_wait(tail.at[layer, k], t_send.at[layer, k])
        else:
            @pl.when((y < Y - 1) | (zh == 0))
            def _():
                send_wait(tail.at[layer, k], t_send.at[layer, k])

            @pl.when((y == Y - 1) & (zh == 0) & (c == 0))
            def _():
                send_wait(tail_relay.at[layer], k_send.at[layer])

    def tail_recv(layer, k):
        def arrive():
            recv_wait(halo.at[layer, k], t_recv.at[layer, k])
            glu[k, 0:HALO, :] = halo[layer, k].astype(jnp.float32)

        if k == 1:
            arrive()
        else:
            @pl.when((y > 0) | (zh > 0))
            def _():
                arrive()

            @pl.when((y == 0) & (zh == 0))
            def _():
                glu[k, 0:HALO, :] = jnp.zeros((HALO, cs), jnp.float32)

    def convolve_tile(layer, k, base):
        first_lane = lax.broadcasted_iota(jnp.int32, (ROWS, 128), 1) == 0
        near = pos[k, pl.ds(base, ROWS), :]
        total = jnp.zeros((ROWS, 128), jnp.float32)
        square = jnp.zeros((ROWS, 128), jnp.float32)
        for t in range(cs // 128):
            at = lanes(h * cs + t * 128, 128)
            span = glu[k, pl.ds(base, ROWS + HALO), t * 128 : (t + 1) * 128]
            acc = jnp.broadcast_to(cbias[layer : layer + 1, at], (ROWS, 128))
            for phase in range(8):
                moved = span if phase == 0 else pltpu.roll(span, ROWS + HALO - phase, 0)
                for off in range(phase, HALO + 1, 8):
                    index = off - (HALO - (WIDTH - 1))
                    if 0 <= index < WIDTH:
                        start = off - phase
                        term = moved[start : start + ROWS] * taps[layer, index : index + 1, at]
                        back = WIDTH - 1 - index
                        acc = acc + (jnp.where(near >= back, term, 0.0) if back else term)
            conv[k, pl.ds(base, ROWS), t * 128 : (t + 1) * 128] = acc
            total = total + acc
            square = square + acc * acc
        s1 = jnp.sum(total, axis=1, keepdims=True)
        s2 = jnp.sum(square, axis=1, keepdims=True)
        stat[k, pl.ds(base, ROWS), :] = jnp.where(first_lane, s1, s2)

    def convolve(layer, k):
        @pl.loop(1, T // ROWS)
        def _(i):
            convolve_tile(layer, k, pl.multiple_of(i * ROWS, ROWS))

    def convolve_first(layer, k):
        convolve_tile(layer, k, 0)
        for t in range(T // 128):
            stat_out[k, :, t * 128 : (t + 1) * 128] = stat[k, t * 128 : (t + 1) * 128, :].T[0:8, :]

    def others():
        for xj in range(X):
            for cj in range(2):
                if xj or cj:
                    device = dev(z, y, (x + xj) % X, (c + cj) % 2)
                    yield xj * 2 + cj, device, (x - xj + X) % X * 2 + (c + cj) % 2

    def stats_send(k):
        for i, device, _ in others():
            send(stat_out.at[k], stat_in.at[k, x * 2 + c], s_send.at[k, i], s_recv.at[k, i], device)

    def row_sum(k):
        for i, _, theirs in others():
            recv_wait(stat_in.at[k, theirs], s_recv.at[k, i])
        stat_in[k, x * 2 + c] = stat_out[k]
        total = stat_in[k, 0]
        for i in range(1, 2 * X):
            total = total + stat_in[k, i]
        stat_row[k, h] = total

        @pl.when(c == 0)
        def _():
            for cc in range(2):
                send(stat_row.at[k, h], stat_row.at[k, h], r_send.at[k, cc], r_recv.at[k], dev(zn, y, x, cc))

    def mix(layer, k):
        recv_wait(stat_row.at[k, 1 - h], r_recv.at[k])
        total = stat_row[k, 0] + stat_row[k, 1]
        for t in range(T // 128):
            tile = total[:, t * 128 : (t + 1) * 128]
            turned = jnp.concatenate([tile] * 16, axis=0).T
            mu = turned[:, 0:1] * (1.0 / C)
            var = turned[:, 1:2] * (1.0 / C) - mu * mu
            rows = slice(t * 128, (t + 1) * 128)
            cols[0, rows, :] = jnp.broadcast_to(mu, (128, 128))
            cols[1, rows, :] = jnp.broadcast_to(lax.rsqrt(var + 1e-5), (128, 128))

        @pl.loop(0, T // ROWS)
        def _(i):
            rows = pl.ds(pl.multiple_of(i * ROWS, ROWS), ROWS)
            mu, scale = cols[0, rows, :], cols[1, rows, :]
            for t in range(cs // 128):
                at = lanes(h * cs + t * 128, 128)
                v = (conv[k, rows, t * 128 : (t + 1) * 128] - mu) * scale
                v = v * cgain[layer : layer + 1, at] + chbias[layer : layer + 1, at]
                mg[k, rows, lanes(me * cs + t * 128, 128)] = jax.nn.silu(v).astype(jnp.bfloat16)

    def stats_sent(k):
        for i, _, _ in others():
            send_wait(stat_out.at[k], s_send.at[k, i])

        @pl.when(c == 0)
        def _():
            for cc in range(2):
                send_wait(stat_row.at[k, h], r_send.at[k, cc])

    def contract(layer, k):
        matmul(branch, mg.at[k], wo_buf.at[layer], C // (Z * Y), Z * Y)
        state[k] = (state[k].astype(jnp.float32) + branch[...]).astype(jnp.bfloat16)

    def docs_start():
        tail_docs = docs.at[pl.ds(T - HALO, HALO)]

        @pl.when(y < Y - 1)
        def _():
            send(tail_docs, doc_halo, d_sem.at[0], d_sem.at[1], dev(z, y + 1, x, c))

        @pl.when((y == Y - 1) & (z < Z - 1))
        def _():
            send(tail_docs, doc_halo, d_sem.at[0], d_sem.at[1], dev(z + 1, 0, x, c))

    def docs_done():
        @pl.when((y > 0) | (z > 0))
        def _():
            recv_wait(doc_halo, d_sem.at[1])

        @pl.when((y == 0) & (z == 0))
        def _():
            doc_halo[...] = jnp.full((HALO, 128), -1, jnp.int32)

        def count(base, span):
            here = span[HALO:]
            total = jnp.zeros((ROWS, 128), jnp.int32)
            for phase in range(8):
                moved = span if phase == 0 else pltpu.roll(span, ROWS + HALO - phase, 0)
                for off in range(phase, HALO, 8):
                    if off >= HALO - (WIDTH - 1):
                        start = off - phase
                        same = moved[start : start + ROWS] == here
                        total = total + jnp.where(same, 1, 0)
            pos[ko, pl.ds(base, ROWS), :] = total

        count(0, jnp.concatenate([doc_halo[...], docs[0:ROWS, :]], axis=0))

        @pl.loop(1, T // ROWS)
        def _(i):
            base = pl.multiple_of(i * ROWS, ROWS)
            count(base, docs[pl.ds(pl.multiple_of(base - HALO, HALO), ROWS + HALO), :])

        @pl.when(c == 0)
        def _():
            send(pos.at[ko], pos.at[ko], d_sem.at[2], d_sem.at[3], dev(zn, y, x, 0))
            send(pos.at[ko], pos.at[ko], d_sem.at[4], d_sem.at[3], dev(zn, y, x, 1))

    def docs_sent():
        @pl.when((y < Y - 1) | (z < Z - 1))
        def _():
            send_wait(doc_halo, d_sem.at[0])

        @pl.when(c == 0)
        def _():
            send_wait(pos.at[ko], d_sem.at[2])
            send_wait(pos.at[ko], d_sem.at[4])

    own0 = xg.at[ko, :, lanes((x * 2 + c) * 2 * ds_, 2 * ds_)]
    local = pltpu.make_async_copy(hid, own0, f_sem.at[0])
    local.start()
    docs_start()

    @pl.when(c == 0)
    def _():
        for q in range(parts):
            hand_over(q)

    start_part(0)

    z_start(0)

    gh = [hidden_gather(0, 0)]
    gh[0].first()
    gh[0].across()
    docs_done()
    event1(0)
    event2(0)
    gh[0].third()
    gh[0].second()
    local.wait()
    z_start(1, 2, kind=0)
    event3(0)
    z_start(1, 2, kind=1)
    start_part(1)

    gm = None
    for layer in range(LAYERS):
        p_now, o_now, p_next = 2 * layer, 2 * layer + 1, 2 * layer + 2
        more = layer + 1 < LAYERS

        def mixed_out(k):
            gm[k].fourth()
            gm[k].last()
            if k == 0:
                part_ready(o_now)
            contract(layer, k)
            if more:
                xg[k, :, lanes(me * ds_, ds_)] = state[k]
                gather = hidden_gather(layer + 1, k)
                gather.first()
                gather.across()
                return gather

        if layer:
            bulk = [o_now, p_next] if more else [o_now]
            z_early(*bulk)
            gh[0].second()
            gh[0].third()
            if layer == 1:
                event2(p_now)
            else:

                @pl.when(inner == 0)
                def _():
                    event2(p_now)

            event3(p_now)
            start_part(o_now)
            gh[1].third()
            if not more:
                gh[1].beyond()
            gh[1].second()
            z_start(*bulk, kind=0)
        for k in range(2):
            if k < len(gh):
                gh[k].fourth()
                gh[k].last()
            if layer and k == 0:
                z_late(*bulk)
            if layer == 0 and k == 0:
                for kk in range(2):
                    state[kk] = xg[kk, :, lanes(me * ds_, ds_)]
            normalise(layer, k)
            if k == 0:
                part_ready(p_now)
            project(layer, k)
            tail[layer, k] = glu[k, T : T + HALO, :].astype(jnp.bfloat16)
            tail_send(layer, k)
            if k < len(gh):
                gh[k].drained()
            if k == 0:
                if layer == 0:
                    recv_wait(pos.at[1 - ko], d_sem.at[3])
                else:
                    stats_sent(0)
                    stats_sent(1)
            convolve(layer, k)
            if k == 0 and layer == 0:
                event1(o_now)

                @pl.when(inner == 1)
                def _():
                    event2(o_now)

        for k in range(2):
            tail_recv(layer, k)
            convolve_first(layer, k)
            if layer:
                gm[k].drained()
            stats_send(k)
        if layer:
            event1(o_now)
            event2(o_now)
        else:

            @pl.when(inner == 0)
            def _():
                event2(o_now)

        for k in range(2):
            row_sum(k)
        gm = [mixed_gather(layer, k) for k in range(2)]
        for k in range(2):
            mix(layer, k)
            gm[k].first()
            gm[k].across()
        event3(o_now)
        if more:
            start_part(p_next)
            if layer == 0:
                event1(p_next)
            else:

                @pl.when(inner == 1)
                def _():
                    event1(p_next)

        gm[0].third()
        gm[0].second()
        gm[1].third()
        if not more:
            gm[1].beyond()
        gm[1].second()
        first = mixed_out(0)
        if more and layer:

            @pl.when(inner == 1)
            def _():
                event2(p_next)

            @pl.when(inner == 0)
            def _():
                event1(p_next)

        gh = [first, mixed_out(1)]

    for k in range(2):
        gm[k].drained()
        stats_sent(k)
    docs_sent()
    half = out.at[:, lanes(h * ds_, ds_)]
    send(state.at[1 - ko], half, f_sem.at[1], f_sem.at[2], zpeer)
    done = pltpu.make_async_copy(state.at[ko], half, f_sem.at[0])
    done.start()
    for layer in range(LAYERS):
        for k in range(2):
            tail_sent(layer, k)
    for q in range(parts):
        part_sent(q)
    send_wait(half, f_sem.at[1])
    done.wait()
    recv_wait(out.at[:, lanes((1 - h) * ds_, ds_)], f_sem.at[2])


def per_device(
    sizes, hidden, doc_ids, norm_gain, w_value, w_gate, conv_taps, conv_bias, chan_gain, chan_bias, w_out
):
    SP, TP = sizes
    Z, Y = grid_of(SP)
    X = TP // 2
    T = hidden.shape[0]
    D = hidden.shape[1] * TP
    C = w_value.shape[2] * TP
    LAYERS, WIDTH = conv_taps.shape[0], conv_taps.shape[1]
    S = 4 * X
    cs, ds_ = C // S, D // S
    rp, ro = D // SP, C // SP
    bf, f32 = jnp.bfloat16, jnp.float32

    docs = jnp.broadcast_to(doc_ids[:, None], (T, 128))

    dims = (Z, Y, X, T, D, C, LAYERS, WIDTH)
    parts = 2 * LAYERS
    nx, ny = X - 1, Y - 1
    dma = pltpu.SemaphoreType.DMA
    vm = pl.BlockSpec(memory_space=pltpu.VMEM)
    hbm = pl.BlockSpec(memory_space=pl.ANY)
    return pl.pallas_call(
        functools.partial(kernel, dims),
        out_shape=jax.ShapeDtypeStruct((T, 2 * ds_), bf),
        in_specs=[hbm, vm, vm, hbm, hbm, vm, vm, vm, vm, hbm],
        out_specs=hbm,
        scratch_shapes=[
            pltpu.VMEM((LAYERS, SP, rp, 2 * cs), bf),
            pltpu.VMEM((LAYERS, SP, ro, ds_), bf),
            pltpu.VMEM((LAYERS, rp, 4 * cs), bf),
            pltpu.VMEM((LAYERS, ro, 2 * ds_), bf),
            pltpu.VMEM((2, T, D), bf),
            pltpu.VMEM((T, D), bf),
            pltpu.VMEM((2, T, C), bf),
            pltpu.VMEM((T, 2 * cs), f32),
            pltpu.VMEM((T, ds_), f32),
            pltpu.VMEM((2, T + HALO, cs), f32),
            pltpu.VMEM((2, T, cs), f32),
            pltpu.VMEM((2, T, ds_), bf),
            pltpu.VMEM((LAYERS, 2, HALO, cs), bf),
            pltpu.VMEM((LAYERS, 2, HALO, cs), bf),
            pltpu.VMEM((2, T, 128), f32),
            pltpu.VMEM((2, 8, T), f32),
            pltpu.VMEM((2, 2 * X, 8, T), f32),
            pltpu.VMEM((2, 2, 8, T), f32),
            pltpu.VMEM((LAYERS, HALO, cs), bf),
            pltpu.VMEM((2, T, 128), f32),
            pltpu.VMEM((2, T, 128), jnp.int32),
            pltpu.VMEM((HALO, 128), jnp.int32),
            dma((parts,)),
            dma((parts,)),
            dma((parts,)),
            dma((parts, 3)),
            dma((parts, Z, ny)),
            dma((parts, 2, 3)),
            dma((parts, Z, ny)),
            dma((2, 3 + 4 * nx)),
            dma((2, 4 + 6 * nx)),
            dma((2, 3 + 4 * nx)),
            dma((2, 4 + 6 * nx)),
            dma((2, 2 * X)),
            dma((2, 2 * X)),
            dma((2,)),
            dma((2, 2)),
            dma((LAYERS,)),
            dma((LAYERS,)),
            dma((LAYERS, 2)),
            dma((LAYERS, 2)),
            dma((3,)),
            dma((5,)),
        ],
        compiler_params=pltpu.CompilerParams(has_side_effects=True, vmem_limit_bytes=60 << 20),
        name="stack",
    )(hidden, docs, norm_gain, w_value, w_gate, conv_taps, conv_bias, chan_gain, chan_bias, w_out)


def solution(mesh):
    placed = (
        P("sp", "tp"),
        P("sp"),
        P(),
        P(None, "sp", "tp"),
        P(None, "sp", "tp"),
        P(None, None, "tp"),
        P(None, "tp"),
        P(None, "tp"),
        P(None, "tp"),
        P(None, "sp", "tp"),
    )
    sizes = (mesh.shape["sp"], mesh.shape["tp"])
    return jax.shard_map(
        functools.partial(per_device, sizes),
        mesh=mesh,
        in_specs=placed,
        out_specs=P("sp", "tp"),
        check_vma=False,
    )
```
